256 devices in a mesh: sp: 128 (over z, y, x), tp: 2 (over core).
Axes of the slice: x: 4, y: 4, z: 8, core: 2. Of those that a mesh axis runs over, the one named last changes fastest.
Arguments:
- conv_value: bfloat16 [65536, 1536], P('sp', 'tp'), may hold values from -6 to 6
- conv_gate: bfloat16 [65536, 1536], P('sp', 'tp'), may hold values from -8 to 8
- conv_out: bfloat16 [65536, 1536], P('sp', 'tp'), may hold values from -40 to 40
- conv_taps: bfloat16 [31, 1536], P(None, 'tp'), may hold values from -1 to 1
- norm_gain: float32 [1536], P('tp'), may hold values from 0.1 to 1.9
- norm_shift: float32 [1536], P('tp'), may hold values from -3 to 3
- proj_weight: bfloat16 [2048, 1536], P(None, 'tp'), may hold values from -0.15625 to 0.15625
- out_grad: bfloat16 [65536, 2048], P('sp'), may hold values from -24 to 24
Outputs:
- grad_value: bfloat16 [65536, 1536], P('sp', 'tp')
- grad_gate: bfloat16 [65536, 1536], P('sp', 'tp')
- grad_taps: float32 [31, 1536], P(None, 'tp')
- grad_gain: float32 [1536], P('tp')
- grad_shift: float32 [1536], P('tp')
- grad_proj: float32 [2048, 1536], P('sp', 'tp')
The draws below stay inside these ranges and needn't reach their ends.
All inputs are finite; a program needn't handle non-finite values.
Results may differ from the reference program's by a relative error of at most 0.005.
Values may be sent and summed in bfloat16 or wider, within the bound.
A program may use at most 64 MiB of HBM per device.

```python
import jax
import jax.numpy as jnp
from jax import lax

D = 2048
CH = 1536
TAPS = 31
SEQ = 65536


def draw_conv_out(key, part):
    key_scale, key_group, key_base, key_mean = jax.random.split(key, 4)
    chan_scale = jnp.exp(jax.random.uniform(key_scale, (CH,), jnp.float32, -1.0, 1.0))
    group_scale = jnp.exp(jax.random.uniform(key_group, (8,), jnp.float32, -1.2, 1.2))
    group_index = jnp.arange(CH) * 8 // CH
    scales = chan_scale * group_scale[group_index]
    base = jax.random.normal(key_base, (SEQ, CH), jnp.float32) * scales
    offset = jax.random.normal(key_mean, (SEQ, 1), jnp.float32)
    return jnp.clip(base + offset, -40.0, 40.0).astype(jnp.bfloat16)


def spiked(values, rng, source, target, parts, factor):
    def block_of(position):
        return (jnp.arange(values.shape[position]) // (values.shape[position] // parts)).reshape((-1,) + (1,) * (values.ndim - 1 - position))

    one_side = jax.random.permutation(rng, parts)[block_of(target)]
    other_side = (block_of(target) + parts // 2) % parts
    return jnp.where((block_of(source) == one_side) | (block_of(source) == other_side), factor * values, values)


def steps_of(stream_key, extent, shards, smallest, high):
    def one(axis_at, parts):
        steps = jax.random.uniform(jax.random.fold_in(jax.random.fold_in(stream_key, 6), axis_at), (parts,), jnp.float32, smallest / len(shards), high / len(shards))
        return jnp.repeat(jnp.exp(steps), extent[axis_at] // parts).reshape((-1,) + (1,) * (len(extent) - axis_at - 1))

    factor_of = one(*shards[0])
    for cut in shards[1:]:
        factor_of = factor_of * one(*cut)
    return factor_of


def bell_draw(own_key, dims, scale, limit, cuts=(), held_as=jnp.bfloat16):
    entries = jax.random.normal(own_key, dims, jnp.float32) * scale
    if len(cuts) > 0:
        entries = steps_of(own_key, dims, cuts, -0.22, 0.18) * entries
    return jnp.clip(entries, min=-limit, max=limit).astype(held_as)


def noise_with(key, extent, spread, reach, pieces, heavy, held_as=jnp.bfloat16):
    drawn = spread * jax.random.normal(key, extent, jnp.float32)
    if pieces:
        drawn = drawn * steps_of(key, extent, pieces, -0.22, 0.18)
    return jnp.clip(spiked(drawn, jax.random.fold_in(key, 3), *heavy), -reach, reach).astype(held_as)


def setup_inputs(seed: int = 0) -> dict:
    splits = jax.random.split(jax.random.key(seed), 9)
    return {
        "conv_value": bell_draw(splits[0], (SEQ, CH), 1.0, 6.0, ((0, 128), (1, 2))),
        "conv_gate": bell_draw(splits[1], (SEQ, CH), 1.5, 8.0, ((0, 128), (1, 2))),
        "conv_out": draw_conv_out(jax.random.fold_in(splits[8], 71), 0),
        "conv_taps": bell_draw(splits[3], (TAPS, CH), TAPS ** -0.5, 1.0, ((1, 2),)),
        "norm_gain": jnp.clip(1.0 + 0.18 * jax.random.normal(splits[4], (CH,), jnp.float32), 0.1, 1.9),
        "norm_shift": bell_draw(splits[5], (CH,), 0.5, 3.0, ((0, 2),), jnp.float32),
        "proj_weight": bell_draw(splits[6], (D, CH), CH ** -0.5, 0.15625, ((1, 2),)),
        "out_grad": noise_with(splits[7], (SEQ, D), 1.0, 24.0, ((0, 128),), (0, 1, 128, 5.5)),
    }


norm_eps = 1e-05

def reference(conv_value, conv_gate, conv_out, conv_taps, norm_gain, norm_shift, proj_weight, out_grad):
    height = conv_out.astype(jnp.float32)
    center = lax.optimization_barrier(jnp.mean(height, axis=1, keepdims=True))
    centered = height - center
    variance = lax.optimization_barrier(jnp.mean(centered * centered, axis=1, keepdims=True))
    inv_std = lax.rsqrt(variance + norm_eps)
    normed = centered * inv_std
    shifted = normed * norm_gain + norm_shift
    sig_norm = jax.nn.sigmoid(shifted)
    active = (shifted * sig_norm).astype(jnp.bfloat16)
    grad_proj = jnp.dot(out_grad.T, active, preferred_element_type=jnp.float32)
    act_grad = jnp.dot(out_grad, proj_weight, preferred_element_type=jnp.float32)
    norm_grad = act_grad * (sig_norm * (1.0 + shifted * (1.0 - sig_norm)))
    grad_gain = lax.optimization_barrier(jnp.sum(norm_grad * normed, axis=0))
    grad_shift = lax.optimization_barrier(jnp.sum(norm_grad, axis=0))
    scaled = norm_grad * norm_gain
    height_grad = inv_std * (scaled - lax.optimization_barrier(jnp.mean(scaled, axis=1, keepdims=True)) - normed * lax.optimization_barrier(jnp.mean(scaled * normed, axis=1, keepdims=True)))
    sig_gate = jax.nn.sigmoid(conv_gate.astype(jnp.float32))
    value_float = conv_value.astype(jnp.float32)
    gated_rows = lax.optimization_barrier((value_float * sig_gate).astype(jnp.bfloat16)).astype(jnp.float32)
    tap_reach = TAPS - 1
    padded_rows = jnp.pad(gated_rows, ((tap_reach, 0), (0, 0)))
    padded_grad = jnp.pad(height_grad, ((0, tap_reach), (0, 0)))
    tap_values = conv_taps.astype(jnp.float32)
    tap_list = []
    gated_grad = jnp.zeros_like(height_grad)
    for tap_index in range(TAPS):
        tap_list.append(lax.optimization_barrier(jnp.sum(height_grad * padded_rows[tap_index:tap_index + SEQ], axis=0)))
        begin = tap_reach - tap_index
        gated_grad = gated_grad + tap_values[tap_index] * padded_grad[begin:begin + SEQ]
    grad_taps = jnp.stack(tap_list)
    grad_value = (gated_grad * sig_gate).astype(jnp.bfloat16)
    grad_gate = (gated_grad * value_float * sig_gate * (1.0 - sig_gate)).astype(jnp.bfloat16)
    return (grad_value, grad_gate, grad_taps, grad_gain, grad_shift, grad_proj)
```

```python
import functools
import types

import jax
import jax.numpy as jnp
from jax import lax
from jax.experimental import pallas as pl
from jax.experimental.pallas import tpu as pltpu
from jax.sharding import PartitionSpec as P

norm_eps = 1e-05
MESH = pl.DeviceIdType.MESH
F32 = jnp.float32
BF16 = jnp.bfloat16
LANES = 128
NX, NY, NZ = 4, 4, 8
PLANE = NX * NY
RING = (NX, NY, NZ)
GROUPS = 3
HALO = 32


def repeat(start, stop, body, unroll):
    assert (stop - start) % unroll == 0

    def step(i, carry):
        for u in range(unroll):
            body(start + i * unroll + u)
        return carry

    lax.fori_loop(0, (stop - start) // unroll, step, 0)


def kernel(names, *refs):
    r = types.SimpleNamespace(**dict(zip(names, refs)))
    rows, chan = r.co.shape
    width = r.og.shape[1]
    n = NX * NY * NZ
    block = width // n
    gcols = chan // GROUPS
    cblocks = chan // LANES
    ntaps = r.taps.shape[0]
    reach = ntaps - 1
    per = r.small_out.shape[0]
    share = r.parts.shape[1]
    chan_total = chan * 2
    me = lax.axis_index("sp")
    core = lax.axis_index("tp")
    x = lax.rem(me, NX)
    y = lax.rem(me // NX, NY)
    z = me // PLANE
    spot = lax.rem(me, PLANE)
    axes = ((x, NX, 1), (y, NY, NX), (z, NZ, PLANE))

    def along(axis, delta):
        c, size, stride = axis
        return me + (lax.rem(c + delta, size) - c) * stride

    def in_plane(i):
        return me - spot + lax.rem(spot + i, PLANE)

    def remote(src, dst, send, recv, device, to_core=None):
        return pltpu.make_async_remote_copy(
            src_ref=src, dst_ref=dst, send_sem=send, recv_sem=recv,
            device_id=(device, core if to_core is None else to_core), device_id_type=MESH,
        )

    loads = [
        pltpu.make_async_copy(src, dst, r.in_sem.at[i])
        for i, (src, dst) in enumerate(
            (
                (r.co_hbm, r.co), (r.og_hbm, r.og), (r.w_hbm, r.w), (r.cg_hbm, r.cg), (r.cv_hbm, r.cv),
                (r.taps_hbm, r.taps), (r.gain_hbm, r.gain), (r.shift_hbm, r.shift),
            )
        )
    ]
    loads[0].start()
    barrier = pltpu.get_barrier_semaphore()

    def greet(device, to_core):
        pl.semaphore_signal(barrier, inc=1, device_id=(device, to_core), device_id_type=MESH)

    greet(me, 1 - core)
    for i in range(1, NZ):
        greet(along(axes[2], i), core)
    for i in range(1, PLANE):
        greet(in_plane(i), core)
    has_prev = me > 0
    has_next = me < n - 1

    @pl.when(has_prev)
    def _():
        greet(me - 1, core)

    @pl.when(has_next)
    def _():
        greet(me + 1, core)

    friends = NZ + PLANE - 1 + has_prev.astype(jnp.int32) + has_next.astype(jnp.int32)

    lane_low = lax.broadcasted_iota(jnp.int32, (1, LANES), 1) < LANES // 2
    nt = rows // LANES
    mid = LANES // 2

    def pack(dst):
        for t in range(nt):
            turned = r.st_a[t * LANES:(t + 1) * LANES, :].T
            dst[0, t:t + 1, :] = turned[:1, :]
            dst[1, t:t + 1, :] = turned[mid:mid + 1, :]

    def unpack(packed, dst):
        for t in range(nt):
            dst[t * LANES:(t + 1) * LANES, :] = jnp.broadcast_to(packed[t:t + 1, :], (LANES, LANES)).T

    def wide(v):
        return jnp.concatenate([v] * cblocks, axis=1)

    for copy in loads[1:]:
        copy.start()
    loads[0].wait()

    def stats(i):
        at = pl.ds(pl.multiple_of(i * 64, 64), 64)
        h = r.co[at, :].astype(F32)
        mean = jnp.sum(h, axis=1, keepdims=True) / chan
        d = h - mean
        m2 = jnp.sum(d * d, axis=1, keepdims=True)
        r.st_a[at, :] = jnp.where(lane_low, mean, m2)

    repeat(0, rows // 64, stats, 2)
    pack(r.pk_a)
    pl.semaphore_wait(barrier, friends)
    swap_a = remote(r.pk_a, r.pk_b, r.tp_send.at[0], r.tp_recv.at[0], me, 1 - core)
    swap_a.start()
    loads[1].wait()
    slab = width // NZ

    def transpose(c, carry):
        t = r.og[:, pl.ds(pl.multiple_of(c * slab, slab), slab)].T
        r.ogt[c] = t.reshape(NY, NX, block, rows)
        return carry

    lax.fori_loop(0, NZ, transpose, 0)
    loads[6].wait()
    loads[7].wait()
    gain = r.gain[...].reshape(1, chan)
    shift = r.shift[...].reshape(1, chan)
    swap_a.wait()
    gap = r.pk_a[0] - r.pk_b[0]
    variance = (r.pk_a[1] + r.pk_b[1] + gap * gap * (0.5 * chan)) / chan_total
    unpack(0.5 * (r.pk_a[0] + r.pk_b[0]), r.st_b)
    unpack(lax.rsqrt(variance + norm_eps), r.st_d)

    def norm(i):
        at = pl.ds(pl.multiple_of(i * 32, 32), 32)
        v = (r.co[at, :].astype(F32) - wide(r.st_b[at, :])) * wide(r.st_d[at, :])
        r.normed[at, :] = v
        t = v * gain + shift
        sig = jax.nn.sigmoid(t)
        r.active[at, :] = (t * sig).astype(BF16)
        r.dsilu[at, :] = sig * (1.0 + t * (1.0 - sig))

    repeat(0, rows // 32, norm, 2)

    acc = (r.acc_a, r.acc_b, r.acc_c)
    sent = (r.sent_a, r.sent_b, r.sent_c)
    came = (r.came_a, r.came_b, r.came_c)
    outer = (NZ, NZ, NY)
    second_axis = (1, 0, 0)
    third_axis = (2, 2, 1)

    def hop(g, d, s, k):
        size = RING[g]
        return remote(
            sent[g].at[d, s, k - 1], came[g].at[d, s, k - 1],
            r.ring_send.at[g, d, s, k - 1], r.ring_recv.at[g, d, s, k - 1],
            along(axes[g], 1 if d == 0 else size - 1),
        )

    def product(g, k):
        size = RING[g]
        far = size // 2
        half = outer[g] // 2
        at = lax.rem(axes[g][0] + k, size)
        lhs = r.ogt[:, :, at] if g == 0 else r.ogt[:, at] if g == 1 else r.ogt[at]
        lhs = lhs.reshape(-1, rows)
        out = jnp.dot(lhs, r.active[:, g * gcols:(g + 1) * gcols], preferred_element_type=F32)
        out = out.reshape(outer[g], 4, block, gcols)
        if k == far:
            for d in range(2):
                sent[g][d, d, far - 1] = out[half * d:half * (d + 1)].astype(BF16)
                hop(g, d, d, far).start()
        elif k in (far - 1, size - far + 1):
            d = 0 if k == far - 1 else 1
            s = 1 - d
            sent[g][d, s, far - 2] = out[half * s:half * (s + 1)].astype(BF16)
            hop(g, d, s, far - 1).start()
            acc[g][k, half * d:half * (d + 1)] = out[half * d:half * (d + 1)]
        else:
            acc[g][k] = out

    def relay(g, d, s, k):
        size = RING[g]
        half = outer[g] // 2
        hop(g, d, s, k).wait_recv()
        at = k - 1 if d == 0 else (size - k + 1) % size
        total = acc[g][at, half * s:half * (s + 1)] + came[g][d, s, k - 1].astype(F32)
        if k > 1:
            sent[g][d, s, k - 2] = total.astype(BF16)
            hop(g, d, s, k - 1).start()
        else:
            acc[g][at, half * s:half * (s + 1)] = total

    def second(g, s, i):
        return remote(
            r.sent2.at[g, s, i - 1, pl.ds(0, outer[g] // 2)], r.came2.at[g, s, i - 1, pl.ds(0, outer[g] // 2)],
            r.second_send.at[g, s, i - 1], r.second_recv.at[g, s, i - 1],
            along(axes[second_axis[g]], i),
        )

    def start_second(g, s):
        half = outer[g] // 2
        c = axes[second_axis[g]][0]
        for i in range(1, 4):
            r.sent2[g, s, i - 1, :half] = acc[g][0, half * s:half * (s + 1), lax.rem(c + i, 4)].astype(BF16)
            second(g, s, i).start()

    def finish_second(g, s):
        half = outer[g] // 2
        c = axes[second_axis[g]][0]
        total = acc[g][0, half * s:half * (s + 1), c]
        for i in range(1, 4):
            second(g, s, i).wait_recv()
            total = total + r.came2[g, s, i - 1, :half].astype(F32)
        r.line[g, half * s:half * (s + 1)] = total

    def third(g, i):
        return remote(
            r.sent3.at[g, i - 1], r.came3.at[g, i - 1],
            r.third_send.at[g, i - 1], r.third_recv.at[g, i - 1],
            along(axes[third_axis[g]], i),
        )

    def start_third(g):
        c, size, _ = axes[third_axis[g]]
        for i in range(1, size):
            r.sent3[g, i - 1] = r.line[g, lax.rem(c + i, size)].astype(BF16)
            third(g, i).start()

    def finish_third(g):
        c, size, _ = axes[third_axis[g]]
        total = r.line[g, c]
        for i in range(1, size):
            third(g, i).wait_recv()
            total = total + r.came3[g, i - 1].astype(F32)
        r.proj_out[:, g * gcols:(g + 1) * gcols] = total

    for g, k in ((0, 2), (1, 2), (2, 4)):
        product(g, k)
    for g, k in ((0, 1), (1, 1), (2, 3), (0, 3), (1, 3), (2, 5)):
        product(g, k)
    for g, k in ((2, 2), (2, 6), (2, 1), (2, 7), (0, 0), (1, 0), (2, 0)):
        product(g, k)
    loads[2].wait()
    r.rowacc[...] = jnp.zeros_like(r.rowacc)

    def act(i, carry):
        at = pl.ds(pl.multiple_of(i * 128, 128), 128)
        r.scaled[at, :] = jnp.dot(r.og[at, :], r.w[...], preferred_element_type=F32)
        return carry

    lax.fori_loop(0, rows // 128, act, 0)
    for d in range(2):
        relay(2, d, d, 4)

    def grads(i):
        at = pl.ds(pl.multiple_of(i * 32, 32), 32)
        v = r.normed[at, :]
        ng = r.scaled[at, :] * r.dsilu[at, :]
        ngz = ng * v
        r.rowacc[0] = r.rowacc[0] + jnp.sum(ngz.reshape(4, 8, chan), axis=0)
        r.rowacc[1] = r.rowacc[1] + jnp.sum(ng.reshape(4, 8, chan), axis=0)
        s = ng * gain
        r.scaled[at, :] = s
        total = jnp.sum(s, axis=1, keepdims=True)
        dot = jnp.sum(s * v, axis=1, keepdims=True)
        r.st_a[at, :] = jnp.where(lane_low, total, dot)

    repeat(0, rows // 32, grads, 2)
    pack(r.pk_c)
    swap_b = remote(r.pk_c, r.pk_d, r.tp_send.at[1], r.tp_recv.at[1], me, 1 - core)
    swap_b.start()
    r.tapacc[...] = jnp.zeros_like(r.tapacc)
    loads[5].wait()
    for c in range(cblocks):
        r.tapf[c] = r.taps[:, c * LANES:(c + 1) * LANES].astype(F32)
    r.flat[...] = jnp.zeros_like(r.flat)
    for g in range(2):
        for d in range(2):
            relay(g, d, d, 2)
    for d in range(2):
        relay(2, d, 1 - d, 3)
    swap_b.wait()
    unpack((r.pk_c[0] + r.pk_d[0]) / chan_total, r.st_a)
    unpack((r.pk_c[1] + r.pk_d[1]) / chan_total, r.st_b)

    def height_rows(i):
        at = pl.ds(pl.multiple_of(i * 32, 32), 32)
        hg = wide(r.st_d[at, :]) * (
            r.scaled[at, :] - wide(r.st_a[at, :]) - r.normed[at, :] * wide(r.st_b[at, :])
        )
        for c in range(cblocks):
            r.hgx[c, at, :] = hg[:, c * LANES:(c + 1) * LANES]
        return hg

    first = height_rows(0)
    for c in range(cblocks):
        r.halo_out[c] = first[:, c * LANES:(c + 1) * LANES].astype(BF16)
    halo_copy = remote(r.halo_out, r.halo_in, r.halo_send, r.halo_recv, lax.rem(me + n - 1, n))

    @pl.when(has_prev)
    def _():
        halo_copy.start()

    repeat(1, rows // 32, height_rows, 3)
    loads[3].wait()
    loads[4].wait()
    for d in range(2):
        relay(2, d, d, 3)
    tall = 128
    talls = rows // tall

    def tap_block(c, q):
        at = pl.ds(q, tall)
        cols = pl.ds(pl.multiple_of(c * LANES, LANES), LANES)
        sig = jax.nn.sigmoid(r.cg[at, cols].astype(F32))
        gated = (r.cv[at, cols].astype(F32) * sig).astype(BF16).astype(F32)
        for j in range(ntaps):
            h = r.hgx[c, pl.ds(q + reach - j, tall), :]
            r.tapacc[c, j] = r.tapacc[c, j] + jnp.sum((gated * h).reshape(tall // 8, 8, LANES), axis=0)

    def inner_taps(lo, hi):
        def body(i, carry):
            tap_block(i // (talls - 1), pl.multiple_of(lax.rem(i, talls - 1) * tall, tall))
            return carry

        lax.fori_loop(lo * (talls - 1), hi * (talls - 1), body, 0)

    inner_taps(0, cblocks // 2)
    for d in range(2):
        relay(2, d, 1 - d, 2)
    for g in range(2):
        for d in range(2):
            relay(g, d, 1 - d, 1)
    for d in range(2):
        relay(2, d, d, 2)
    inner_taps(cblocks // 2, cblocks)

    @pl.when(has_next)
    def _():
        halo_copy.wait_recv()
        r.hgx[:, rows:, :] = r.halo_in[...].astype(F32)

    @pl.when(jnp.logical_not(has_next))
    def _():
        r.hgx[:, rows:, :] = jnp.zeros((cblocks, HALO, LANES), F32)


    def last_tap(c, carry):
        tap_block(c, rows - tall)
        return carry

    lax.fori_loop(0, cblocks, last_tap, 0)
    for c in range(cblocks):
        r.flat[c * per:c * per + ntaps, :] = jnp.sum(r.tapacc[c], axis=1)
        for j in range(2):
            r.flat[c * per + ntaps + j:c * per + ntaps + j + 1, :] = jnp.sum(
                r.rowacc[j, :, c * LANES:(c + 1) * LANES], axis=0, keepdims=True
            )

    def piece(ref, i):
        return ref.at[pl.ds(pl.multiple_of(i * share, share), share)]

    def scatter(i):
        return remote(
            piece(r.flat, lax.rem(spot + i, PLANE)), r.parts.at[i - 1],
            r.a_send.at[i - 1], r.a_recv.at[i - 1], in_plane(i),
        )

    def deep(i, sender):
        return remote(
            r.pile.at[z], r.pile.at[sender], r.b_send.at[i - 1], r.b_recv.at[sender], along(axes[2], i),
        )

    def gather(i, sender):
        return remote(
            piece(r.whole, spot), piece(r.whole, sender), r.c_send.at[i - 1], r.c_recv.at[sender], in_plane(i),
        )

    for i in range(1, PLANE):
        scatter(i).start()
    for g in range(2):
        for d in range(2):
            relay(g, d, d, 1)
    for g in range(2):
        for s in range(2):
            start_second(g, s)
    for d in range(2):
        relay(2, d, 1 - d, 1)
    for d in range(2):
        relay(2, d, d, 1)
    for s in range(2):
        start_second(2, s)
    step = 64
    steps = rows // step

    def grad_block(i, carry):
        c = i // steps
        q = pl.multiple_of(lax.rem(i, steps) * step, step)
        at = pl.ds(q, step)
        cols = pl.ds(pl.multiple_of(c * LANES, LANES), LANES)
        sig = jax.nn.sigmoid(r.cg[at, cols].astype(F32))
        value = r.cv[at, cols].astype(F32)
        total = jnp.zeros((step, LANES), F32)
        for j in range(ntaps):
            total = total + r.tapf[c, pl.ds(j, 1), :] * r.hgx[c, pl.ds(q + reach - j, step), :]
        r.gv[at, cols] = (total * sig).astype(BF16)
        r.gg[at, cols] = (total * value * sig * (1.0 - sig)).astype(BF16)
        return carry

    lax.fori_loop(0, 3 * steps, grad_block, 0)
    mine = piece(r.flat, spot)[...]
    for i in range(1, PLANE):
        scatter(i).wait_recv()
        mine = mine + r.parts[i - 1]
    r.pile[z] = mine
    for i in range(1, NZ):
        deep(i, z).start()
    for g in range(2):
        for s in range(2):
            finish_second(g, s)
        start_third(g)
    lax.fori_loop(3 * steps, 5 * steps, grad_block, 0)
    for i in range(1, NZ):
        deep(i, lax.rem(z + i, NZ)).wait_recv()
    mine = r.pile[0]
    for i in range(1, NZ):
        mine = mine + r.pile[i]
    piece(r.whole, spot)[...] = mine
    for i in range(1, PLANE):
        gather(i, spot).start()
    for s in range(2):
        finish_second(2, s)
    start_third(2)
    lax.fori_loop(5 * steps, cblocks * steps, grad_block, 0)
    stores = [
        pltpu.make_async_copy(src, dst, r.out_sem.at[i])
        for i, (src, dst) in enumerate(((r.gv, r.gv_hbm), (r.gg, r.gg_hbm)))
    ]
    for copy in stores:
        copy.start()
    finish_third(0)
    finish_third(1)
    finish_third(2)
    for i in range(1, PLANE):
        gather(i, lax.rem(spot + i, PLANE)).wait_recv()
    for c in range(cblocks):
        r.small_out[:, c * LANES:(c + 1) * LANES] = r.whole[c * per:(c + 1) * per, :]
    for g in range(GROUPS):
        far = RING[g] // 2
        for d in range(2):
            for s in range(2):
                for k in range(1, far + (1 if s == d else 0)):
                    hop(g, d, s, k).wait_send()
        for s in range(2):
            for i in range(1, 4):
                second(g, s, i).wait_send()
        for i in range(1, axes[third_axis[g]][1]):
            third(g, i).wait_send()
    for i in range(1, PLANE):
        scatter(i).wait_send()
        gather(i, spot).wait_send()
    for i in range(1, NZ):
        deep(i, z).wait_send()

    @pl.when(has_prev)
    def _():
        halo_copy.wait_send()

    for copy in stores:
        copy.wait()


def place(gv_in, gg_in, small, proj_in, gv_out, gg_out, taps, gain, shift, proj_out, gv, gg, proj, in_sem, out_sem):
    ins = [
        pltpu.make_async_copy(src, dst, in_sem.at[i])
        for i, (src, dst) in enumerate(((gv_in, gv), (gg_in, gg), (proj_in, proj)))
    ]
    outs = [
        pltpu.make_async_copy(src, dst, out_sem.at[i])
        for i, (src, dst) in enumerate(((gv, gv_out), (gg, gg_out), (proj, proj_out)))
    ]
    for copy in ins:
        copy.start()
    ntaps = taps.shape[0]
    taps[...] = small[:ntaps, :]
    gain[...] = small[ntaps, :]
    shift[...] = small[ntaps + 1, :]
    for came, goes in zip(ins, outs):
        came.wait()
        goes.start()
    for copy in outs:
        copy.wait()


def local(conv_value, conv_gate, conv_out, conv_taps, norm_gain, norm_shift, proj_weight, out_grad):
    rows, chan = conv_value.shape
    ntaps = conv_taps.shape[0]
    width = out_grad.shape[1]
    n = lax.axis_size("sp")
    assert n == NX * NY * NZ and lax.axis_size("tp") == 2
    gcols = chan // GROUPS
    block = width // n
    cblocks = chan // LANES
    per = -(-(ntaps + 2) // 8) * 8
    share = -(-(-(-per * cblocks // PLANE)) // 8) * 8
    hbm = pl.BlockSpec(memory_space=pl.ANY)
    vmem = pl.BlockSpec(memory_space=pltpu.VMEM)
    dma = pltpu.SemaphoreType.DMA

    def ring_buffer(size, deep):
        return pltpu.VMEM((2, 2, size // 2, deep // 2, 4, block, gcols), BF16)

    scratch = dict(
        cv=pltpu.VMEM((rows, chan), BF16),
        cg=pltpu.VMEM((rows, chan), BF16),
        co=pltpu.VMEM((rows, chan), BF16),
        w=pltpu.VMEM((width, chan), BF16),
        og=pltpu.VMEM((rows, width), BF16),
        taps=pltpu.VMEM((ntaps, chan), BF16),
        gain=pltpu.VMEM((chan,), F32),
        shift=pltpu.VMEM((chan,), F32),
        ogt=pltpu.VMEM((NZ, NY, NX, block, rows), BF16),
        active=pltpu.VMEM((rows, chan), BF16),
        normed=pltpu.VMEM((rows, chan), F32),
        dsilu=pltpu.VMEM((rows, chan), F32),
        scaled=pltpu.VMEM((rows, chan), F32),
        hgx=pltpu.VMEM((cblocks, rows + HALO, LANES), F32),
        gv=pltpu.VMEM((rows, chan), BF16),
        gg=pltpu.VMEM((rows, chan), BF16),
        st_a=pltpu.VMEM((rows, LANES), F32),
        st_b=pltpu.VMEM((rows, LANES), F32),
        st_d=pltpu.VMEM((rows, LANES), F32),
        pk_a=pltpu.VMEM((2, rows // LANES, LANES), F32),
        pk_b=pltpu.VMEM((2, rows // LANES, LANES), F32),
        pk_c=pltpu.VMEM((2, rows // LANES, LANES), F32),
        pk_d=pltpu.VMEM((2, rows // LANES, LANES), F32),
        tapf=pltpu.VMEM((cblocks, ntaps, LANES), F32),
        tapacc=pltpu.VMEM((cblocks, ntaps, 8, LANES), F32),
        rowacc=pltpu.VMEM((2, 8, chan), F32),
        halo_out=pltpu.VMEM((cblocks, HALO, LANES), BF16),
        halo_in=pltpu.VMEM((cblocks, HALO, LANES), BF16),
        acc_a=pltpu.VMEM((NX, NZ, 4, block, gcols), F32),
        acc_b=pltpu.VMEM((NY, NZ, 4, block, gcols), F32),
        acc_c=pltpu.VMEM((NZ, NY, 4, block, gcols), F32),
        sent_a=ring_buffer(NX, NZ),
        sent_b=ring_buffer(NY, NZ),
        sent_c=ring_buffer(NZ, NY),
        came_a=ring_buffer(NX, NZ),
        came_b=ring_buffer(NY, NZ),
        came_c=ring_buffer(NZ, NY),
        sent2=pltpu.VMEM((GROUPS, 2, 3, NZ // 2, block, gcols), BF16),
        came2=pltpu.VMEM((GROUPS, 2, 3, NZ // 2, block, gcols), BF16),
        line=pltpu.VMEM((GROUPS, NZ, block, gcols), F32),
        sent3=pltpu.VMEM((GROUPS, NZ - 1, block, gcols), BF16),
        came3=pltpu.VMEM((GROUPS, NZ - 1, block, gcols), BF16),
        flat=pltpu.VMEM((PLANE * share, LANES), F32),
        parts=pltpu.VMEM((PLANE - 1, share, LANES), F32),
        pile=pltpu.VMEM((NZ, share, LANES), F32),
        whole=pltpu.VMEM((PLANE * share, LANES), F32),
        in_sem=dma((8,)),
        out_sem=dma((2,)),
        tp_send=dma((2,)),
        tp_recv=dma((2,)),
        halo_send=dma,
        halo_recv=dma,
        ring_send=dma((GROUPS, 2, 2, NZ // 2)),
        ring_recv=dma((GROUPS, 2, 2, NZ // 2)),
        second_send=dma((GROUPS, 2, 3)),
        second_recv=dma((GROUPS, 2, 3)),
        third_send=dma((GROUPS, NZ - 1)),
        third_recv=dma((GROUPS, NZ - 1)),
        a_send=dma((PLANE - 1,)),
        a_recv=dma((PLANE - 1,)),
        b_send=dma((NZ - 1,)),
        b_recv=dma((NZ,)),
        c_send=dma((PLANE - 1,)),
        c_recv=dma((PLANE,)),
    )
    ins = ("cv_hbm", "cg_hbm", "co_hbm", "taps_hbm", "gain_hbm", "shift_hbm", "w_hbm", "og_hbm")
    outs = ("gv_hbm", "gg_hbm", "small_out", "proj_out")
    grad_value, grad_gate, small, grad_proj = pl.pallas_call(
        functools.partial(kernel, (*ins, *outs, *scratch)),
        out_shape=(
            jax.ShapeDtypeStruct((rows, chan), BF16),
            jax.ShapeDtypeStruct((rows, chan), BF16),
            jax.ShapeDtypeStruct((per, chan), F32),
            jax.ShapeDtypeStruct((block, chan), F32),
        ),
        in_specs=[hbm] * 8,
        out_specs=(hbm, hbm, vmem, vmem),
        scratch_shapes=list(scratch.values()),
        compiler_params=pltpu.CompilerParams(
            collective_id=0, has_side_effects=True, vmem_limit_bytes=60 * 1024 * 1024
        ),
    )(
        conv_value, conv_gate, conv_out, conv_taps, norm_gain, norm_shift, proj_weight, out_grad,
    )
    return pl.pallas_call(
        place,
        out_shape=(
            jax.ShapeDtypeStruct((rows, chan), BF16),
            jax.ShapeDtypeStruct((rows, chan), BF16),
            jax.ShapeDtypeStruct((ntaps, chan), F32),
            jax.ShapeDtypeStruct((chan,), F32),
            jax.ShapeDtypeStruct((chan,), F32),
            jax.ShapeDtypeStruct((block, chan), F32),
        ),
        in_specs=[hbm, hbm, vmem, hbm],
        out_specs=(hbm, hbm, vmem, vmem, vmem, hbm),
        scratch_shapes=[
            pltpu.VMEM((rows, chan), BF16),
            pltpu.VMEM((rows, chan), BF16),
            pltpu.VMEM((block, chan), F32),
            dma((3,)), dma((3,)),
        ],
    )(grad_value, grad_gate, small, grad_proj)


def solution(mesh):
    in_specs = (
        P("sp", "tp"),
        P("sp", "tp"),
        P("sp", "tp"),
        P(None, "tp"),
        P("tp"),
        P("tp"),
        P(None, "tp"),
        P("sp", None),
    )
    out_specs = (P("sp", "tp"), P("sp", "tp"), P(None, "tp"), P("tp"), P("tp"), P("sp", "tp"))
    return jax.shard_map(local, mesh=mesh, in_specs=in_specs, out_specs=out_specs, check_vma=False)
```

```python
import functools
import types

import jax
import jax.numpy as jnp
from jax import lax
from jax.experimental import pallas as pl
from jax.experimental.pallas import tpu as pltpu
from jax.sharding import PartitionSpec as P

norm_eps = 1e-05
MESH = pl.DeviceIdType.MESH
F32 = jnp.float32
BF16 = jnp.bfloat16
LANES = 128
NX, NY, NZ = 4, 4, 8
PLANE = NX * NY
RING = (NX, NY, NZ)
GROUPS = 3
HALO = 32
VMEM_LIMIT = 48 * 1024 * 1024


def repeat(start, stop, body, unroll):
    assert (stop - start) % unroll == 0

    def step(i, carry):
        for u in range(unroll):
            body(start + i * unroll + u)
        return carry

    lax.fori_loop(0, (stop - start) // unroll, step, 0)


def kernel(names, *refs):
    r = types.SimpleNamespace(**dict(zip(names, refs)))
    rows, chan = r.co.shape
    width = r.og.shape[1]
    n = NX * NY * NZ
    block = width // n
    gcols = chan // GROUPS
    cblocks = chan // LANES
    ntaps = r.taps.shape[0]
    reach = ntaps - 1
    per = -(-(ntaps + 2) // 8) * 8
    share = r.parts.shape[1]
    chan_total = chan * 2
    me = lax.axis_index("sp")
    core = lax.axis_index("tp")
    x = lax.rem(me, NX)
    y = lax.rem(me // NX, NY)
    z = me // PLANE
    spot = lax.rem(me, PLANE)
    axes = ((x, NX, 1), (y, NY, NX), (z, NZ, PLANE))

    def along(axis, delta):
        c, size, stride = axis
        return me + (lax.rem(c + delta, size) - c) * stride

    def in_plane(i):
        return me - spot + lax.rem(spot + i, PLANE)

    def remote(src, dst, send, recv, device, to_core=None):
        return pltpu.make_async_remote_copy(
            src_ref=src, dst_ref=dst, send_sem=send, recv_sem=recv,
            device_id=(device, core if to_core is None else to_core), device_id_type=MESH,
        )

    loads = [
        pltpu.make_async_copy(src, dst, r.in_sem.at[i])
        for i, (src, dst) in enumerate(
            (
                (r.co_hbm, r.co), (r.og_hbm, r.og), (r.w_hbm, r.w), (r.cg_hbm, r.cg), (r.cv_hbm, r.cv),
                (r.taps_hbm, r.taps), (r.gain_hbm, r.gain), (r.shift_hbm, r.shift),
            )
        )
    ]
    loads[0].start()
    barrier = pltpu.get_barrier_semaphore()

    def greet(device, to_core):
        pl.semaphore_signal(barrier, inc=1, device_id=(device, to_core), device_id_type=MESH)

    greet(me, 1 - core)
    for i in range(1, NZ):
        greet(along(axes[2], i), core)
    for i in range(1, PLANE):
        greet(in_plane(i), core)
    has_prev = me > 0
    has_next = me < n - 1

    @pl.when(has_prev)
    def _():
        greet(me - 1, core)

    @pl.when(has_next)
    def _():
        greet(me + 1, core)

    friends = NZ + PLANE - 1 + has_prev.astype(jnp.int32) + has_next.astype(jnp.int32)

    lane_low = lax.broadcasted_iota(jnp.int32, (1, LANES), 1) < LANES // 2
    nt = rows // LANES
    mid = LANES // 2

    def pack(dst):
        for t in range(nt):
            turned = r.st_a[t * LANES:(t + 1) * LANES, :].T
            dst[0, t:t + 1, :] = turned[:1, :]
            dst[1, t:t + 1, :] = turned[mid:mid + 1, :]

    def unpack(packed, dst):
        for t in range(nt):
            dst[t * LANES:(t + 1) * LANES, :] = jnp.broadcast_to(packed[t:t + 1, :], (LANES, LANES)).T

    def wide(v):
        return jnp.concatenate([v] * cblocks, axis=1)

    for copy in loads[1:]:
        copy.start()
    loads[0].wait()

    def stats(i):
        at = pl.ds(pl.multiple_of(i * 64, 64), 64)
        h = r.co[at, :].astype(F32)
        mean = jnp.sum(h, axis=1, keepdims=True) / chan
        d = h - mean
        m2 = jnp.sum(d * d, axis=1, keepdims=True)
        r.st_a[at, :] = jnp.where(lane_low, mean, m2)

    repeat(0, rows // 64, stats, 2)
    pack(r.pk_a)
    pl.semaphore_wait(barrier, friends)
    swap_a = remote(r.pk_a, r.pk_b, r.tp_send.at[0], r.tp_recv.at[0], me, 1 - core)
    swap_a.start()
    loads[1].wait()
    slab = width // NZ

    def transpose(c, carry):
        t = r.og[:, pl.ds(pl.multiple_of(c * slab, slab), slab)].T
        r.ogt[c] = t.reshape(NY, NX, block, rows)
        return carry

    lax.fori_loop(0, NZ, transpose, 0)
    loads[6].wait()
    loads[7].wait()
    gain = r.gain[...].reshape(1, chan)
    shift = r.shift[...].reshape(1, chan)
    swap_a.wait()
    gap = r.pk_a[0] - r.pk_b[0]
    variance = (r.pk_a[1] + r.pk_b[1] + gap * gap * (0.5 * chan)) / chan_total
    unpack(0.5 * (r.pk_a[0] + r.pk_b[0]), r.st_b)
    unpack(lax.rsqrt(variance + norm_eps), r.st_d)

    def norm(i):
        at = pl.ds(pl.multiple_of(i * 32, 32), 32)
        v = (r.co[at, :].astype(F32) - wide(r.st_b[at, :])) * wide(r.st_d[at, :])
        r.normed[at, :] = v
        t = v * gain + shift
        sig = jax.nn.sigmoid(t)
        r.active[at, :] = (t * sig).astype(BF16)
        r.dsilu[at, :] = sig * (1.0 + t * (1.0 - sig))

    repeat(0, rows // 32, norm, 2)

    acc = (r.acc_a, r.acc_b, r.acc_c)
    sent = (r.sent_a, r.sent_b, r.sent_c)
    came = (r.came_a, r.came_b, r.came_c)
    sent2 = (r.sent2_a, r.sent2_b, r.sent2_c)
    came2 = (r.came2_a, r.came2_b, r.came2_c)
    sent3 = (r.sent3_a, r.sent3_b, r.sent3_c)
    came3 = (r.came3_a, r.came3_b, r.came3_c)
    outer = (NZ, NZ, NY)
    second_axis = (1, 0, 0)
    third_axis = (2, 2, 1)
    first_recv = (0, 2 * NX - 2, 2 * NX + 2 * NY - 4)

    def slot(g, d, s, k):
        far = RING[g] // 2
        return d * (2 * far - 1) + (k - 1 if s == d else far + k - 1)

    def hop(g, d, s, k):
        i = slot(g, d, s, k)
        return remote(
            sent[g].at[i], came[g].at[i], r.ring_send.at[g], r.ring_recv.at[first_recv[g] + i],
            along(axes[g], 1 if d == 0 else RING[g] - 1),
        )

    def product(g, k):
        size = RING[g]
        far = size // 2
        half = outer[g] // 2
        at = lax.rem(axes[g][0] + k, size)
        lhs = r.ogt[:, :, at] if g == 0 else r.ogt[:, at] if g == 1 else r.ogt[at]
        lhs = lhs.reshape(-1, rows)
        out = jnp.dot(lhs, r.active[:, g * gcols:(g + 1) * gcols], preferred_element_type=F32)
        out = out.reshape(outer[g], 4, block, gcols)
        if k == far:
            for d in range(2):
                sent[g][slot(g, d, d, far)] = out[half * d:half * (d + 1)].astype(BF16)
        elif k in (far - 1, size - far + 1):
            d = 0 if k == far - 1 else 1
            s = 1 - d
            sent[g][slot(g, d, s, far - 1)] = out[half * s:half * (s + 1)].astype(BF16)
            acc[g][k, half * d:half * (d + 1)] = out[half * d:half * (d + 1)]
        else:
            acc[g][k] = out

    def launch(g, own):
        far = RING[g] // 2
        for d in range(2):
            if own:
                hop(g, d, 1 - d, far - 1).start()
            else:
                hop(g, d, d, far).start()

    def relay(g, d, s, k):
        size = RING[g]
        half = outer[g] // 2
        hop(g, d, s, k).wait_recv()
        at = k - 1 if d == 0 else (size - k + 1) % size
        total = acc[g][at, half * s:half * (s + 1)] + came[g][slot(g, d, s, k)].astype(F32)
        if k > 1:
            sent[g][slot(g, d, s, k - 1)] = total.astype(BF16)
            hop(g, d, s, k - 1).start()
        else:
            acc[g][at, half * s:half * (s + 1)] = total

    def start_second(g, s):
        half = outer[g] // 2
        c = axes[second_axis[g]][0]
        for i in range(1, 4):
            sent2[g][s, i - 1] = acc[g][0, half * s:half * (s + 1), lax.rem(c + i, 4)].astype(BF16)
            remote(
                sent2[g].at[s, i - 1], came2[g].at[s, i - 1],
                r.second_send.at[g], r.second_recv.at[g, s], along(axes[second_axis[g]], i),
            ).start()

    def finish_second(g, s):
        half = outer[g] // 2
        c = axes[second_axis[g]][0]
        remote(sent2[g].at[s], came2[g].at[s], r.second_send.at[g], r.second_recv.at[g, s], me).wait_recv()
        total = acc[g][0, half * s:half * (s + 1), c]
        for i in range(1, 4):
            total = total + came2[g][s, i - 1].astype(F32)
        r.line[g, half * s:half * (s + 1)] = total

    def start_third(g):
        c, size, _ = axes[third_axis[g]]
        for i in range(1, size):
            sent3[g][i - 1] = r.line[g, lax.rem(c + i, size)].astype(BF16)
            remote(
                sent3[g].at[i - 1], came3[g].at[i - 1],
                r.third_send.at[g], r.third_recv.at[g], along(axes[third_axis[g]], i),
            ).start()

    def finish_third(g):
        c, size, _ = axes[third_axis[g]]
        remote(sent3[g], came3[g], r.third_send.at[g], r.third_recv.at[g], me).wait_recv()
        total = r.line[g, c]
        for i in range(1, size):
            total = total + came3[g][i - 1].astype(F32)
        r.proj_out[:, g * gcols:(g + 1) * gcols] = total

    for g, k in ((0, 2), (1, 2), (2, 4)):
        product(g, k)
    for g in range(GROUPS):
        launch(g, False)
    for g, k in ((0, 1), (0, 3), (1, 1), (1, 3), (2, 3), (2, 5)):
        product(g, k)
    for g in range(GROUPS):
        launch(g, True)
    for g, k in ((2, 2), (2, 6), (2, 1), (2, 7), (0, 0), (1, 0), (2, 0)):
        product(g, k)
    loads[2].wait()
    r.rowacc[...] = jnp.zeros_like(r.rowacc)

    def act(i, carry):
        cols = pl.ds(pl.multiple_of(i * gcols, gcols), gcols)
        r.scaled[:, cols] = jnp.dot(r.og[...], r.w[:, cols], preferred_element_type=F32)
        return carry

    lax.fori_loop(0, GROUPS, act, 0)
    for d in range(2):
        relay(2, d, d, 4)

    def grads(i):
        at = pl.ds(pl.multiple_of(i * 32, 32), 32)
        v = r.normed[at, :]
        ng = r.scaled[at, :] * r.dsilu[at, :]
        ngz = ng * v
        r.rowacc[0] = r.rowacc[0] + jnp.sum(ngz.reshape(4, 8, chan), axis=0)
        r.rowacc[1] = r.rowacc[1] + jnp.sum(ng.reshape(4, 8, chan), axis=0)
        s = ng * gain
        r.scaled[at, :] = s
        total = jnp.sum(s, axis=1, keepdims=True)
        dot = jnp.sum(s * v, axis=1, keepdims=True)
        r.st_a[at, :] = jnp.where(lane_low, total, dot)

    repeat(0, rows // 32, grads, 2)
    pack(r.pk_c)
    swap_b = remote(r.pk_c, r.pk_d, r.tp_send.at[1], r.tp_recv.at[1], me, 1 - core)
    swap_b.start()
    r.tapacc[...] = jnp.zeros_like(r.tapacc)
    loads[5].wait()
    for c in range(cblocks):
        r.tapf[c] = r.taps[:, c * LANES:(c + 1) * LANES].astype(F32)
    r.flat[...] = jnp.zeros_like(r.flat)
    for g in range(2):
        for d in range(2):
            relay(g, d, d, 2)
    for d in range(2):
        relay(2, d, 1 - d, 3)
    swap_b.wait()
    unpack((r.pk_c[0] + r.pk_d[0]) / chan_total, r.st_a)
    unpack((r.pk_c[1] + r.pk_d[1]) / chan_total, r.st_b)

    def height_rows(i):
        at = pl.ds(pl.multiple_of(i * 32, 32), 32)
        hg = wide(r.st_d[at, :]) * (
            r.scaled[at, :] - wide(r.st_a[at, :]) - r.normed[at, :] * wide(r.st_b[at, :])
        )
        for c in range(cblocks):
            r.hgx[c, at, :] = hg[:, c * LANES:(c + 1) * LANES]
        return hg

    first = height_rows(0)
    for c in range(cblocks):
        r.halo_out[c] = first[:, c * LANES:(c + 1) * LANES].astype(BF16)
    halo_copy = remote(r.halo_out, r.halo_in, r.halo_send, r.halo_recv, lax.rem(me + n - 1, n))

    @pl.when(has_prev)
    def _():
        halo_copy.start()

    repeat(1, rows // 32, height_rows, 3)
    loads[3].wait()
    loads[4].wait()
    tall = 128
    talls = rows // tall

    def tap_block(c, q):
        at = pl.ds(q, tall)
        cols = pl.ds(pl.multiple_of(c * LANES, LANES), LANES)
        sig = jax.nn.sigmoid(r.cg[at, cols].astype(F32))
        gated = (r.cv[at, cols].astype(F32) * sig).astype(BF16).astype(F32)
        for j in range(ntaps):
            h = r.hgx[c, pl.ds(q + reach - j, tall), :]
            r.tapacc[c, j] = r.tapacc[c, j] + jnp.sum((gated * h).reshape(tall // 8, 8, LANES), axis=0)

    def inner_taps(lo, hi):
        def body(i, carry):
            tap_block(i // (talls - 1), pl.multiple_of(lax.rem(i, talls - 1) * tall, tall))
            return carry

        lax.fori_loop(lo * (talls - 1), hi * (talls - 1), body, 0)

    inner_taps(0, cblocks // 2)
    for d in range(2):
        relay(2, d, d, 3)
    inner_taps(cblocks // 2, cblocks)

    @pl.when(has_next)
    def _():
        halo_copy.wait_recv()
        r.hgx[:, rows:, :] = r.halo_in[...].astype(F32)

    @pl.when(jnp.logical_not(has_next))
    def _():
        r.hgx[:, rows:, :] = jnp.zeros((cblocks, HALO, LANES), F32)


    def last_tap(c, carry):
        tap_block(c, rows - tall)
        return carry

    lax.fori_loop(0, cblocks, last_tap, 0)
    for c in range(cblocks):
        r.flat[c * per:c * per + ntaps, :] = jnp.sum(r.tapacc[c], axis=1)
        for j in range(2):
            r.flat[c * per + ntaps + j:c * per + ntaps + j + 1, :] = jnp.sum(
                r.rowacc[j, :, c * LANES:(c + 1) * LANES], axis=0, keepdims=True
            )

    def piece(i):
        return r.flat.at[pl.ds(pl.multiple_of(i * share, share), share)]

    for i in range(1, PLANE):
        remote(
            piece(lax.rem(spot + i, PLANE)), r.parts.at[i - 1], r.a_send, r.a_recv, in_plane(i),
        ).start()
    for g in range(2):
        for d in range(2):
            relay(g, d, 1 - d, 1)
    for d in range(2):
        relay(2, d, 1 - d, 2)
    for g in range(2):
        for d in range(2):
            relay(g, d, d, 1)
    for g in range(2):
        for s in range(2):
            start_second(g, s)
    step = 64
    steps = rows // step

    def grad_block(i, carry):
        c = i // steps
        q = pl.multiple_of(lax.rem(i, steps) * step, step)
        at = pl.ds(q, step)
        cols = pl.ds(pl.multiple_of(c * LANES, LANES), LANES)
        sig = jax.nn.sigmoid(r.cg[at, cols].astype(F32))
        value = r.cv[at, cols].astype(F32)
        total = jnp.zeros((step, LANES), F32)
        for j in range(ntaps):
            total = total + r.tapf[c, pl.ds(j, 1), :] * r.hgx[c, pl.ds(q + reach - j, step), :]
        r.gv[at, cols] = (total * sig).astype(BF16)
        r.gg[at, cols] = (total * value * sig * (1.0 - sig)).astype(BF16)
        return carry

    lax.fori_loop(0, 2 * steps, grad_block, 0)
    for d in range(2):
        relay(2, d, d, 2)
    lax.fori_loop(2 * steps, 4 * steps, grad_block, 0)
    remote(r.parts, r.parts, r.a_send, r.a_recv, me).wait_recv()
    mine = piece(spot)[...]
    for i in range(1, PLANE):
        mine = mine + r.parts[i - 1]
    r.pile[NZ - 1] = mine
    for i in range(1, NZ):
        remote(r.pile.at[NZ - 1], r.pile.at[i - 1], r.b_send, r.b_recv, along(axes[2], i)).start()
    for g in range(2):
        for s in range(2):
            finish_second(g, s)
        start_third(g)
    for d in range(2):
        relay(2, d, 1 - d, 1)
    for d in range(2):
        relay(2, d, d, 1)
    for s in range(2):
        start_second(2, s)
    lax.fori_loop(4 * steps, cblocks * steps, grad_block, 0)
    nearby = r.pile.at[pl.ds(0, NZ - 1)]
    remote(nearby, nearby, r.b_send, r.b_recv, me).wait_recv()
    mine = r.pile[lax.rem(z + NZ - 1, NZ)]
    for i in range(1, NZ):
        mine = mine + r.pile[lax.rem(z - i + 2 * NZ - 1, NZ)]
    r.whole[PLANE - 1] = mine
    for i in range(1, PLANE):
        remote(r.whole.at[PLANE - 1], r.whole.at[i - 1], r.c_send, r.c_recv, in_plane(i)).start()
    for s in range(2):
        finish_second(2, s)
    start_third(2)
    finish_third(0)
    finish_third(1)
    around = r.whole.at[pl.ds(0, PLANE - 1)]
    remote(around, around, r.c_send, r.c_recv, me).wait_recv()
    gains, shifts = [], []
    for c in range(cblocks):
        cols = slice(c * LANES, (c + 1) * LANES)
        for m in range(0, per, 8):
            row = c * per + m
            seg = r.whole[lax.rem(spot - row // share + 2 * PLANE - 1, PLANE), row % share:row % share + 8]
            for q in range(m, m + 8):
                if q == ntaps:
                    gains.append(seg[q - m:q - m + 1])
                elif q == ntaps + 1:
                    shifts.append(seg[q - m:q - m + 1])
            if m < ntaps:
                end = min(m + 8, ntaps)
                r.taps_out[m:end, cols] = seg[:end - m]
    r.gain_out[...] = jnp.concatenate(gains, axis=1).reshape(chan)
    r.shift_out[...] = jnp.concatenate(shifts, axis=1).reshape(chan)
    finish_third(2)
    for g in range(GROUPS):
        remote(sent[g], came[g], r.ring_send.at[g], r.ring_recv.at[0], me).wait_send()
        remote(sent2[g], came2[g], r.second_send.at[g], r.second_recv.at[g, 0], me).wait_send()
        remote(sent3[g], came3[g], r.third_send.at[g], r.third_recv.at[g], me).wait_send()
    remote(r.parts, r.parts, r.a_send, r.a_recv, me).wait_send()
    remote(nearby, nearby, r.b_send, r.b_recv, me).wait_send()
    remote(around, around, r.c_send, r.c_recv, me).wait_send()

    @pl.when(has_prev)
    def _():
        halo_copy.wait_send()


def place(*refs):
    arrays = (len(refs) - 1) // 2
    copies = [
        pltpu.make_async_copy(refs[i], refs[arrays + i], refs[-1].at[i]) for i in range(arrays)
    ]
    for copy in copies:
        copy.start()
    for copy in copies:
        copy.wait()


def local(conv_value, conv_gate, conv_out, conv_taps, norm_gain, norm_shift, proj_weight, out_grad):
    rows, chan = conv_value.shape
    ntaps = conv_taps.shape[0]
    width = out_grad.shape[1]
    n = lax.axis_size("sp")
    assert n == NX * NY * NZ and lax.axis_size("tp") == 2
    gcols = chan // GROUPS
    block = width // n
    cblocks = chan // LANES
    per = -(-(ntaps + 2) // 8) * 8
    share = -(-(-(-per * cblocks // PLANE)) // 8) * 8
    hbm = pl.BlockSpec(memory_space=pl.ANY)
    vmem = pl.BlockSpec(memory_space=pltpu.VMEM)
    dma = pltpu.SemaphoreType.DMA

    def ring_buffer(size, deep):
        return pltpu.VMEM((2 * size - 2, deep // 2, 4, block, gcols), BF16)

    def pieces(*lead):
        return pltpu.VMEM((*lead, block, gcols), BF16)

    scratch = dict(
        cv=pltpu.VMEM((rows, chan), BF16),
        cg=pltpu.VMEM((rows, chan), BF16),
        co=pltpu.VMEM((rows, chan), BF16),
        w=pltpu.VMEM((width, chan), BF16),
        og=pltpu.VMEM((rows, width), BF16),
        taps=pltpu.VMEM((ntaps, chan), BF16),
        gain=pltpu.VMEM((chan,), F32),
        shift=pltpu.VMEM((chan,), F32),
        ogt=pltpu.VMEM((NZ, NY, NX, block, rows), BF16),
        active=pltpu.VMEM((rows, chan), BF16),
        normed=pltpu.VMEM((rows, chan), F32),
        dsilu=pltpu.VMEM((rows, chan), F32),
        scaled=pltpu.VMEM((rows, chan), F32),
        hgx=pltpu.VMEM((cblocks, rows + HALO, LANES), F32),
        st_a=pltpu.VMEM((rows, LANES), F32),
        st_b=pltpu.VMEM((rows, LANES), F32),
        st_d=pltpu.VMEM((rows, LANES), F32),
        pk_a=pltpu.VMEM((2, rows // LANES, LANES), F32),
        pk_b=pltpu.VMEM((2, rows // LANES, LANES), F32),
        pk_c=pltpu.VMEM((2, rows // LANES, LANES), F32),
        pk_d=pltpu.VMEM((2, rows // LANES, LANES), F32),
        tapf=pltpu.VMEM((cblocks, ntaps, LANES), F32),
        tapacc=pltpu.VMEM((cblocks, ntaps, 8, LANES), F32),
        rowacc=pltpu.VMEM((2, 8, chan), F32),
        halo_out=pltpu.VMEM((cblocks, HALO, LANES), BF16),
        halo_in=pltpu.VMEM((cblocks, HALO, LANES), BF16),
        acc_a=pltpu.VMEM((NX, NZ, 4, block, gcols), F32),
        acc_b=pltpu.VMEM((NY, NZ, 4, block, gcols), F32),
        acc_c=pltpu.VMEM((NZ, NY, 4, block, gcols), F32),
        sent_a=ring_buffer(NX, NZ),
        sent_b=ring_buffer(NY, NZ),
        sent_c=ring_buffer(NZ, NY),
        came_a=ring_buffer(NX, NZ),
        came_b=ring_buffer(NY, NZ),
        came_c=ring_buffer(NZ, NY),
        sent2_a=pieces(2, 3, NZ // 2),
        sent2_b=pieces(2, 3, NZ // 2),
        sent2_c=pieces(2, 3, NY // 2),
        came2_a=pieces(2, 3, NZ // 2),
        came2_b=pieces(2, 3, NZ // 2),
        came2_c=pieces(2, 3, NY // 2),
        line=pltpu.VMEM((GROUPS, NZ, block, gcols), F32),
        sent3_a=pieces(NZ - 1),
        sent3_b=pieces(NZ - 1),
        sent3_c=pieces(NY - 1),
        came3_a=pieces(NZ - 1),
        came3_b=pieces(NZ - 1),
        came3_c=pieces(NY - 1),
        flat=pltpu.VMEM((PLANE * share, LANES), F32),
        parts=pltpu.VMEM((PLANE - 1, share, LANES), F32),
        pile=pltpu.VMEM((NZ, share, LANES), F32),
        whole=pltpu.VMEM((PLANE, share, LANES), F32),
        in_sem=dma((8,)),
        tp_send=dma((2,)),
        tp_recv=dma((2,)),
        halo_send=dma,
        halo_recv=dma,
        ring_send=dma((GROUPS,)),
        ring_recv=dma((2 * (NX + NY + NZ) - 6,)),
        second_send=dma((GROUPS,)),
        second_recv=dma((GROUPS, 2)),
        third_send=dma((GROUPS,)),
        third_recv=dma((GROUPS,)),
        a_send=dma,
        a_recv=dma,
        b_send=dma,
        b_recv=dma,
        c_send=dma,
        c_recv=dma,
    )
    ins = ("cv_hbm", "cg_hbm", "co_hbm", "taps_hbm", "gain_hbm", "shift_hbm", "w_hbm", "og_hbm")
    outs = dict(
        gv=((rows, chan), BF16),
        gg=((rows, chan), BF16),
        taps_out=((ntaps, chan), F32),
        gain_out=((chan,), F32),
        shift_out=((chan,), F32),
        proj_out=((block, chan), F32),
    )
    results = pl.pallas_call(
        functools.partial(kernel, (*ins, *outs, *scratch)),
        out_shape=[pltpu.VMEM(*out) for out in outs.values()],
        in_specs=[pl.BlockSpec(memory_space=pltpu.HBM)] * 8,
        out_specs=[vmem] * len(outs),
        scratch_shapes=list(scratch.values()),
        compiler_params=pltpu.CompilerParams(
            collective_id=0, has_side_effects=True, vmem_limit_bytes=VMEM_LIMIT
        ),
    )(
        *[
            pltpu.with_memory_space_constraint(v, pltpu.HBM)
            for v in (
                conv_value, conv_gate, conv_out, conv_taps, norm_gain, norm_shift, proj_weight, out_grad,
            )
        ]
    )
    return pl.pallas_call(
        place,
        out_shape=[jax.ShapeDtypeStruct(*out) for out in outs.values()],
        in_specs=[vmem] * len(outs),
        out_specs=[hbm] * len(outs),
        scratch_shapes=[dma((len(outs),))],
        compiler_params=pltpu.CompilerParams(vmem_limit_bytes=1024 * 1024),
    )(*[pltpu.with_memory_space_constraint(v, pltpu.VMEM) for v in results])


def solution(mesh):
    in_specs = (
        P("sp", "tp"),
        P("sp", "tp"),
        P("sp", "tp"),
        P(None, "tp"),
        P("tp"),
        P("tp"),
        P(None, "tp"),
        P("sp", None),
    )
    out_specs = (P("sp", "tp"), P("sp", "tp"), P(None, "tp"), P("tp"), P("tp"), P("sp", "tp"))
    return jax.shard_map(local, mesh=mesh, in_specs=in_specs, out_specs=out_specs, check_vma=False)
```

```python
import functools
import types

import jax
import jax.numpy as jnp
from jax import lax
from jax.experimental import pallas as pl
from jax.experimental.pallas import tpu as pltpu
from jax.sharding import PartitionSpec as P

norm_eps = 1e-05
MESH = pl.DeviceIdType.MESH
F32 = jnp.float32
BF16 = jnp.bfloat16
LANES = 128
NX, NY, NZ = 4, 4, 8
PLANE = NX * NY
RING = (NX, NY, NZ)
GROUPS = 3
HALO = 32
VMEM_LIMIT = 48 * 1024 * 1024


def repeat(start, stop, body, unroll):
    assert (stop - start) % unroll == 0

    def step(i, carry):
        for u in range(unroll):
            body(start + i * unroll + u)
        return carry

    lax.fori_loop(0, (stop - start) // unroll, step, 0)


def kernel(names, *refs):
    r = types.SimpleNamespace(**dict(zip(names, refs)))
    rows, chan = r.co.shape
    width = r.og.shape[1]
    n = NX * NY * NZ
    block = width // n
    gcols = chan // GROUPS
    cblocks = chan // LANES
    ntaps = r.taps.shape[0]
    reach = ntaps - 1
    per = -(-(ntaps + 2) // 8) * 8
    share = r.parts.shape[1]
    chan_total = chan * 2
    me = lax.axis_index("sp")
    core = lax.axis_index("tp")
    x = lax.rem(me, NX)
    y = lax.rem(me // NX, NY)
    z = me // PLANE
    spot = lax.rem(me, PLANE)
    axes = ((x, NX, 1), (y, NY, NX), (z, NZ, PLANE))

    def along(axis, delta):
        c, size, stride = axis
        return me + (lax.rem(c + delta, size) - c) * stride

    def in_plane(i):
        return me - spot + lax.rem(spot + i, PLANE)

    def remote(src, dst, send, recv, device, to_core=None):
        return pltpu.make_async_remote_copy(
            src_ref=src, dst_ref=dst, send_sem=send, recv_sem=recv,
            device_id=(device, core if to_core is None else to_core), device_id_type=MESH,
        )

    loads = [
        pltpu.make_async_copy(src, dst, r.in_sem.at[i])
        for i, (src, dst) in enumerate(
            (
                (r.co_hbm, r.co), (r.og_hbm, r.og), (r.w_hbm, r.w), (r.cg_hbm, r.cg), (r.cv_hbm, r.cv),
                (r.taps_hbm, r.taps), (r.gain_hbm, r.gain), (r.shift_hbm, r.shift),
            )
        )
    ]
    loads[0].start()
    barrier = pltpu.get_barrier_semaphore()

    def greet(device, to_core):
        pl.semaphore_signal(barrier, inc=1, device_id=(device, to_core), device_id_type=MESH)

    greet(me, 1 - core)
    for i in range(1, NZ):
        greet(along(axes[2], i), core)
    for i in range(1, PLANE):
        greet(in_plane(i), core)
    has_prev = me > 0
    has_next = me < n - 1

    @pl.when(has_prev)
    def _():
        greet(me - 1, core)

    @pl.when(has_next)
    def _():
        greet(me + 1, core)

    friends = NZ + PLANE - 1 + has_prev.astype(jnp.int32) + has_next.astype(jnp.int32)

    lane_low = lax.broadcasted_iota(jnp.int32, (1, LANES), 1) < LANES // 2
    nt = rows // LANES
    mid = LANES // 2

    def pack(dst):
        for t in range(nt):
            turned = r.st_a[t * LANES:(t + 1) * LANES, :].T
            dst[0, t:t + 1, :] = turned[:1, :]
            dst[1, t:t + 1, :] = turned[mid:mid + 1, :]

    def unpack(packed, dst):
        for t in range(nt):
            dst[t * LANES:(t + 1) * LANES, :] = jnp.broadcast_to(packed[t:t + 1, :], (LANES, LANES)).T

    def wide(v):
        return jnp.concatenate([v] * cblocks, axis=1)

    for copy in loads[1:]:
        copy.start()
    loads[0].wait()

    def stats(i):
        at = pl.ds(pl.multiple_of(i * 64, 64), 64)
        h = r.co[at, :].astype(F32)
        mean = jnp.sum(h, axis=1, keepdims=True) / chan
        d = h - mean
        m2 = jnp.sum(d * d, axis=1, keepdims=True)
        r.st_a[at, :] = jnp.where(lane_low, mean, m2)

    repeat(0, rows // 64, stats, 2)
    pack(r.pk_a)
    pl.semaphore_wait(barrier, friends)
    swap_a = remote(r.pk_a, r.pk_b, r.tp_send.at[0], r.tp_recv.at[0], me, 1 - core)
    swap_a.start()
    loads[1].wait()
    slab = width // NZ

    def transpose(c, carry):
        t = r.og[:, pl.ds(pl.multiple_of(c * slab, slab), slab)].T
        r.ogt[c] = t.reshape(NY, NX, block, rows)
        return carry

    lax.fori_loop(0, NZ, transpose, 0)
    loads[3].wait()
    loads[4].wait()

    def gate_rows(i):
        at = pl.ds(pl.multiple_of(i * 32, 32), 32)
        value = r.cv[at, :].astype(F32)
        return (value * jax.nn.sigmoid(r.cg[at, :].astype(F32))).astype(BF16)

    r.gate_out[...] = gate_rows(rows // HALO - 1)
    gate_copy = remote(r.gate_out, r.gate_in, r.gate_send, r.gate_recv, lax.rem(me + 1, n))

    @pl.when(has_next)
    def _():
        gate_copy.start()

    loads[6].wait()
    loads[7].wait()
    gain = r.gain[...].reshape(1, chan)
    shift = r.shift[...].reshape(1, chan)
    swap_a.wait()
    gap = r.pk_a[0] - r.pk_b[0]
    variance = (r.pk_a[1] + r.pk_b[1] + gap * gap * (0.5 * chan)) / chan_total
    unpack(0.5 * (r.pk_a[0] + r.pk_b[0]), r.st_b)
    unpack(lax.rsqrt(variance + norm_eps), r.st_d)

    def norm(i):
        at = pl.ds(pl.multiple_of(i * 32, 32), 32)
        v = (r.co[at, :].astype(F32) - wide(r.st_b[at, :])) * wide(r.st_d[at, :])
        r.normed[at, :] = v
        t = v * gain + shift
        sig = jax.nn.sigmoid(t)
        r.active[at, :] = (t * sig).astype(BF16)
        r.dsilu[at, :] = sig * (1.0 + t * (1.0 - sig))

    repeat(0, rows // 32, norm, 2)

    acc = (r.acc_a, r.acc_b, r.acc_c)
    sent = (r.sent_a, r.sent_b, r.sent_c)
    came = (r.came_a, r.came_b, r.came_c)
    sent2 = (r.sent2_a, r.sent2_b)
    came2 = (r.came2_a, r.came2_b)
    sent3 = (r.sent3_a, r.sent3_b)
    came3 = (r.came3_a, r.came3_b)
    outer = (NZ, NZ, NY)
    second_axis = (1, 0)
    third_axis = (2, 2)
    first_recv = (0, 2 * NX - 2, 2 * NX + 2 * NY - 4)

    def slot(g, d, s, k):
        far = RING[g] // 2
        return d * (2 * far - 1) + (k - 1 if s == d else far + k - 1)

    def hop(g, d, s, k):
        i = slot(g, d, s, k)
        return remote(
            sent[g].at[i], came[g].at[i], r.ring_send.at[g], r.ring_recv.at[first_recv[g] + i],
            along(axes[g], 1 if d == 0 else RING[g] - 1),
        )

    def product(g, k):
        size = RING[g]
        far = size // 2
        half = outer[g] // 2
        at = lax.rem(axes[g][0] + k, size)
        lhs = r.ogt[:, :, at] if g == 0 else r.ogt[:, at] if g == 1 else r.ogt[at]
        lhs = lhs.reshape(-1, rows)
        out = jnp.dot(lhs, r.active[:, g * gcols:(g + 1) * gcols], preferred_element_type=F32)
        out = out.reshape(outer[g], 4, block, gcols)
        if k == far:
            for d in range(2):
                sent[g][slot(g, d, d, far)] = out[half * d:half * (d + 1)].astype(BF16)
        elif k in (far - 1, size - far + 1):
            d = 0 if k == far - 1 else 1
            s = 1 - d
            sent[g][slot(g, d, s, far - 1)] = out[half * s:half * (s + 1)].astype(BF16)
            acc[g][k, half * d:half * (d + 1)] = out[half * d:half * (d + 1)]
        else:
            acc[g][k] = out

    def launch(g, own):
        far = RING[g] // 2
        for d in range(2):
            if own:
                hop(g, d, 1 - d, far - 1).start()
            else:
                hop(g, d, d, far).start()

    def relay(g, d, s, k):
        size = RING[g]
        half = outer[g] // 2
        hop(g, d, s, k).wait_recv()
        at = k - 1 if d == 0 else (size - k + 1) % size
        total = acc[g][at, half * s:half * (s + 1)] + came[g][slot(g, d, s, k)].astype(F32)
        if k > 1:
            sent[g][slot(g, d, s, k - 1)] = total.astype(BF16)
            hop(g, d, s, k - 1).start()
        else:
            acc[g][at, half * s:half * (s + 1)] = total

    def start_plane():
        for i in range(1, PLANE):
            peer = lax.rem(spot + i, PLANE)
            r.sent_p[i - 1] = acc[2][0, peer // NX, lax.rem(peer, NX)].astype(BF16)
            remote(r.sent_p.at[i - 1], r.came_p.at[i - 1], r.plane_send, r.plane_recv, in_plane(i)).start()

    def finish_plane():
        remote(r.sent_p, r.came_p, r.plane_send, r.plane_recv, me).wait_recv()
        total = acc[2][0, y, x]
        for i in range(1, PLANE):
            total = total + r.came_p[i - 1].astype(F32)
        r.proj_out[:, 2 * gcols:] = total

    def start_second(g, s):
        half = outer[g] // 2
        c = axes[second_axis[g]][0]
        for i in range(1, 4):
            sent2[g][s, i - 1] = acc[g][0, half * s:half * (s + 1), lax.rem(c + i, 4)].astype(BF16)
            remote(
                sent2[g].at[s, i - 1], came2[g].at[s, i - 1],
                r.second_send.at[g], r.second_recv.at[g, s], along(axes[second_axis[g]], i),
            ).start()

    def finish_second(g, s):
        half = outer[g] // 2
        c = axes[second_axis[g]][0]
        remote(sent2[g].at[s], came2[g].at[s], r.second_send.at[g], r.second_recv.at[g, s], me).wait_recv()
        total = acc[g][0, half * s:half * (s + 1), c]
        for i in range(1, 4):
            total = total + came2[g][s, i - 1].astype(F32)
        r.line[g, half * s:half * (s + 1)] = total

    def start_third(g):
        c, size, _ = axes[third_axis[g]]
        for i in range(1, size):
            sent3[g][i - 1] = r.line[g, lax.rem(c + i, size)].astype(BF16)
            remote(
                sent3[g].at[i - 1], came3[g].at[i - 1],
                r.third_send.at[g], r.third_recv.at[g], along(axes[third_axis[g]], i),
            ).start()

    def finish_third(g):
        c, size, _ = axes[third_axis[g]]
        remote(sent3[g], came3[g], r.third_send.at[g], r.third_recv.at[g], me).wait_recv()
        total = r.line[g, c]
        for i in range(1, size):
            total = total + came3[g][i - 1].astype(F32)
        r.proj_out[:, g * gcols:(g + 1) * gcols] = total

    for g, k in ((2, 4), (0, 2), (1, 2)):
        product(g, k)
    for g in (2, 0, 1):
        launch(g, False)
    for g, k in ((2, 3), (2, 5), (0, 1), (0, 3), (1, 1), (1, 3)):
        product(g, k)
    for g in (2, 0, 1):
        launch(g, True)
    loads[2].wait()

    def act(i):
        cols = slice(i * gcols, (i + 1) * gcols)
        r.scaled[:, cols] = jnp.dot(r.og[...], r.w[:, cols], preferred_element_type=F32)

    def grads(i):
        cols = slice(i * gcols, (i + 1) * gcols)
        sums = [jnp.zeros((8, gcols), F32)] * 2
        for q in range(0, rows, 32):
            at = slice(q, q + 32)
            v = r.normed[at, cols]
            ng = r.scaled[at, cols] * r.dsilu[at, cols]
            sums = [
                sums[0] + jnp.sum((ng * v).reshape(4, 8, gcols), axis=0),
                sums[1] + jnp.sum(ng.reshape(4, 8, gcols), axis=0),
            ]
            s = ng * gain[:, cols]
            r.scaled[at, cols] = s
            for dst, t in ((r.st_a, s), (r.st_b, s * v)):
                t = t[:, :LANES] + t[:, LANES:]
                dst[at, :] = t if i == 0 else dst[at, :] + t
        for j in range(2):
            r.rowacc[j, :, cols] = sums[j]

    act(0)
    for i in range(1, GROUPS):
        act(i)
        grads(i - 1)
    grads(GROUPS - 1)

    def fold(i):
        at = pl.ds(pl.multiple_of(i * 64, 64), 64)
        total = jnp.sum(r.st_a[at, :], axis=1, keepdims=True)
        dot = jnp.sum(r.st_b[at, :], axis=1, keepdims=True)
        r.st_a[at, :] = jnp.where(lane_low, total, dot)

    repeat(0, rows // 64, fold, 2)
    pack(r.pk_c)
    swap_b = remote(r.pk_c, r.pk_d, r.tp_send.at[1], r.tp_recv.at[1], me, 1 - core)
    swap_b.start()
    r.tapacc[...] = jnp.zeros_like(r.tapacc)
    loads[5].wait()
    for c in range(cblocks):
        r.tapf[c] = r.taps[:, c * LANES:(c + 1) * LANES].astype(F32)
    r.flat[...] = jnp.zeros_like(r.flat)
    for d in range(2):
        relay(2, d, d, 4)

    def gate(i):
        at = pl.ds(pl.multiple_of(HALO + i * 32, 32), 32)
        gated = gate_rows(i).astype(F32)
        for c in range(cblocks):
            r.gx[c, at, :] = gated[:, c * LANES:(c + 1) * LANES]

    repeat(0, rows // 32, gate, 2)

    @pl.when(has_prev)
    def _():
        gate_copy.wait_recv()
        for c in range(cblocks):
            r.gx[c, :HALO, :] = r.gate_in[:, c * LANES:(c + 1) * LANES].astype(F32)

    @pl.when(jnp.logical_not(has_prev))
    def _():
        r.gx[:, :HALO, :] = jnp.zeros((cblocks, HALO, LANES), F32)

    for k in (2, 6):
        product(2, k)
    swap_b.wait()
    unpack((r.pk_c[0] + r.pk_d[0]) / chan_total, r.st_a)
    unpack((r.pk_c[1] + r.pk_d[1]) / chan_total, r.st_b)

    def height_rows(i):
        at = pl.ds(pl.multiple_of(i * 32, 32), 32)
        hg = wide(r.st_d[at, :]) * (
            r.scaled[at, :] - wide(r.st_a[at, :]) - r.normed[at, :] * wide(r.st_b[at, :])
        )
        for c in range(cblocks):
            r.hgx[c, at, :] = hg[:, c * LANES:(c + 1) * LANES]
        return hg

    first = height_rows(0)
    for c in range(cblocks):
        r.halo_out[c] = first[:, c * LANES:(c + 1) * LANES].astype(BF16)
    halo_copy = remote(r.halo_out, r.halo_in, r.halo_send, r.halo_recv, lax.rem(me + n - 1, n))

    @pl.when(has_prev)
    def _():
        halo_copy.start()

    repeat(1, rows // 32, height_rows, 3)
    for g in range(2):
        for d in range(2):
            relay(g, d, d, 2)
    for d in range(2):
        relay(2, d, 1 - d, 3)
    tall = 128
    talls = rows // tall
    skip = HALO - reach

    def tap_block(i, carry):
        c = i // talls
        q = pl.multiple_of(lax.rem(i, talls) * tall, tall)
        hg = r.hgx[c, pl.ds(q, tall), :]
        for m in range(8):
            js = range(m, ntaps, 8)
            near = r.gx[c, pl.ds(q + skip + m, tall + 8 * (len(js) - 1)), :]
            for k, j in enumerate(js):
                both = near[8 * k:8 * k + tall] * hg
                r.tapacc[c, j] = r.tapacc[c, j] + jnp.sum(both.reshape(tall // 8, 8, LANES), axis=0)
        return carry

    early = 16
    lax.fori_loop(0, early, tap_block, 0)
    for d in range(2):
        relay(2, d, d, 3)
    lax.fori_loop(early, cblocks * talls, tap_block, 0)
    for c in range(cblocks):
        r.flat[c * per:c * per + ntaps, :] = jnp.sum(r.tapacc[c], axis=1)
        for j in range(2):
            r.flat[c * per + ntaps + j:c * per + ntaps + j + 1, :] = jnp.sum(
                r.rowacc[j, :, c * LANES:(c + 1) * LANES], axis=0, keepdims=True
            )

    def piece(i):
        return r.flat.at[pl.ds(pl.multiple_of(i * share, share), share)]

    for i in range(1, PLANE):
        remote(
            piece(lax.rem(spot + i, PLANE)), r.parts.at[i - 1], r.a_send, r.a_recv, in_plane(i),
        ).start()
    for g, k in ((0, 0), (1, 0), (2, 1), (2, 7), (2, 0)):
        product(g, k)
    for g in range(2):
        for d in range(2):
            relay(g, d, 1 - d, 1)
    for g in range(2):
        for d in range(2):
            relay(g, d, d, 1)
    for g in range(2):
        for s in range(2):
            start_second(g, s)
    step = 64
    steps = rows // step

    def grad_block(i, carry):
        inner = i < cblocks * (steps - 1)
        c = jnp.where(inner, i // (steps - 1), i - cblocks * (steps - 1))
        q = pl.multiple_of(jnp.where(inner, lax.rem(i, steps - 1), steps - 1) * step, step)
        at = pl.ds(q, step)
        cols = pl.ds(pl.multiple_of(c * LANES, LANES), LANES)
        sig = jax.nn.sigmoid(r.cg[at, cols].astype(F32))
        value = r.cv[at, cols].astype(F32)
        total = jnp.zeros((step, LANES), F32)
        for m in range(8):
            ks = range(m, ntaps, 8)
            near = r.hgx[c, pl.ds(q + m, step + 8 * (len(ks) - 1)), :]
            for k, j in enumerate(ks):
                total = total + r.tapf[c, pl.ds(reach - j, 1), :] * near[8 * k:8 * k + step]
        r.gv[at, cols] = (total * sig).astype(BF16)
        r.gg[at, cols] = (total * value * sig * (1.0 - sig)).astype(BF16)
        return carry

    lax.fori_loop(0, 7, grad_block, 0)
    for d in range(2):
        relay(2, d, 1 - d, 2)
    for d in range(2):
        relay(2, d, d, 2)
    lax.fori_loop(7, 28, grad_block, 0)
    remote(r.parts, r.parts, r.a_send, r.a_recv, me).wait_recv()
    mine = piece(spot)[...]
    for i in range(1, PLANE):
        mine = mine + r.parts[i - 1]
    r.pile[NZ - 1] = mine
    for i in range(1, NZ):
        remote(r.pile.at[NZ - 1], r.pile.at[i - 1], r.b_send, r.b_recv, along(axes[2], i)).start()
    lax.fori_loop(28, 36, grad_block, 0)
    for d in range(2):
        relay(2, d, 1 - d, 1)
    for d in range(2):
        relay(2, d, d, 1)
    start_plane()
    for g in range(2):
        for s in range(2):
            finish_second(g, s)
        start_third(g)

    @pl.when(has_next)
    def _():
        halo_copy.wait_recv()
        r.hgx[:, rows:, :] = r.halo_in[...].astype(F32)

    @pl.when(jnp.logical_not(has_next))
    def _():
        r.hgx[:, rows:, :] = jnp.zeros((cblocks, HALO, LANES), F32)

    lax.fori_loop(36, cblocks * steps, grad_block, 0)
    nearby = r.pile.at[pl.ds(0, NZ - 1)]
    remote(nearby, nearby, r.b_send, r.b_recv, me).wait_recv()
    mine = r.pile[lax.rem(z + NZ - 1, NZ)]
    for i in range(1, NZ):
        mine = mine + r.pile[lax.rem(z - i + 2 * NZ - 1, NZ)]
    r.whole[PLANE - 1] = mine.astype(BF16)
    for i in range(1, PLANE):
        remote(r.whole.at[PLANE - 1], r.whole.at[i - 1], r.c_send, r.c_recv, in_plane(i)).start()
    finish_third(0)
    finish_third(1)
    around = r.whole.at[pl.ds(0, PLANE - 1)]
    remote(around, around, r.c_send, r.c_recv, me).wait_recv()
    gains, shifts = [], []
    for c in range(cblocks):
        cols = slice(c * LANES, (c + 1) * LANES)
        for m in range(0, per, 8):
            row = c * per + m
            seg = r.whole[lax.rem(spot - row // share + 2 * PLANE - 1, PLANE)].astype(F32)
            seg = seg[row % share:row % share + 8]
            for q in range(m, m + 8):
                if q == ntaps:
                    gains.append(seg[q - m:q - m + 1])
                elif q == ntaps + 1:
                    shifts.append(seg[q - m:q - m + 1])
            if m < ntaps:
                end = min(m + 8, ntaps)
                r.taps_out[m:end, cols] = seg[:end - m]
    r.gain_out[...] = jnp.concatenate(gains, axis=1).reshape(chan)
    r.shift_out[...] = jnp.concatenate(shifts, axis=1).reshape(chan)
    finish_plane()
    for g in range(GROUPS):
        remote(sent[g], came[g], r.ring_send.at[g], r.ring_recv.at[0], me).wait_send()
    for g in range(2):
        remote(sent2[g], came2[g], r.second_send.at[g], r.second_recv.at[g, 0], me).wait_send()
        remote(sent3[g], came3[g], r.third_send.at[g], r.third_recv.at[g], me).wait_send()
    remote(r.sent_p, r.came_p, r.plane_send, r.plane_recv, me).wait_send()
    remote(r.parts, r.parts, r.a_send, r.a_recv, me).wait_send()
    remote(nearby, nearby, r.b_send, r.b_recv, me).wait_send()
    remote(around, around, r.c_send, r.c_recv, me).wait_send()

    @pl.when(has_prev)
    def _():
        halo_copy.wait_send()

    @pl.when(has_next)
    def _():
        gate_copy.wait_send()


def place(*refs):
    arrays = (len(refs) - 1) // 2
    copies = [
        pltpu.make_async_copy(refs[i], refs[arrays + i], refs[-1].at[i]) for i in range(arrays)
    ]
    for copy in copies:
        copy.start()
    for copy in copies:
        copy.wait()


def local(conv_value, conv_gate, conv_out, conv_taps, norm_gain, norm_shift, proj_weight, out_grad):
    rows, chan = conv_value.shape
    ntaps = conv_taps.shape[0]
    width = out_grad.shape[1]
    n = lax.axis_size("sp")
    assert n == NX * NY * NZ and lax.axis_size("tp") == 2
    gcols = chan // GROUPS
    block = width // n
    cblocks = chan // LANES
    per = -(-(ntaps + 2) // 8) * 8
    share = -(-(-(-per * cblocks // PLANE)) // 8) * 8
    hbm = pl.BlockSpec(memory_space=pl.ANY)
    vmem = pl.BlockSpec(memory_space=pltpu.VMEM)
    dma = pltpu.SemaphoreType.DMA

    def ring_buffer(size, deep):
        return pltpu.VMEM((2 * size - 2, deep // 2, 4, block, gcols), BF16)

    def pieces(*lead):
        return pltpu.VMEM((*lead, block, gcols), BF16)

    scratch = dict(
        cv=pltpu.VMEM((rows, chan), BF16),
        cg=pltpu.VMEM((rows, chan), BF16),
        co=pltpu.VMEM((rows, chan), BF16),
        w=pltpu.VMEM((width, chan), BF16),
        og=pltpu.VMEM((rows, width), BF16),
        taps=pltpu.VMEM((ntaps, chan), BF16),
        gain=pltpu.VMEM((chan,), F32),
        shift=pltpu.VMEM((chan,), F32),
        ogt=pltpu.VMEM((NZ, NY, NX, block, rows), BF16),
        active=pltpu.VMEM((rows, chan), BF16),
        normed=pltpu.VMEM((rows, chan), F32),
        dsilu=pltpu.VMEM((rows, chan), F32),
        scaled=pltpu.VMEM((rows, chan), F32),
        hgx=pltpu.VMEM((cblocks, rows + HALO, LANES), F32),
        st_a=pltpu.VMEM((rows, LANES), F32),
        st_b=pltpu.VMEM((rows, LANES), F32),
        st_d=pltpu.VMEM((rows, LANES), F32),
        pk_a=pltpu.VMEM((2, rows // LANES, LANES), F32),
        pk_b=pltpu.VMEM((2, rows // LANES, LANES), F32),
        pk_c=pltpu.VMEM((2, rows // LANES, LANES), F32),
        pk_d=pltpu.VMEM((2, rows // LANES, LANES), F32),
        tapf=pltpu.VMEM((cblocks, ntaps, LANES), F32),
        tapacc=pltpu.VMEM((cblocks, ntaps, 8, LANES), F32),
        rowacc=pltpu.VMEM((2, 8, chan), F32),
        gx=pltpu.VMEM((cblocks, HALO + rows, LANES), F32),
        gate_out=pltpu.VMEM((HALO, chan), BF16),
        gate_in=pltpu.VMEM((HALO, chan), BF16),
        halo_out=pltpu.VMEM((cblocks, HALO, LANES), BF16),
        halo_in=pltpu.VMEM((cblocks, HALO, LANES), BF16),
        acc_a=pltpu.VMEM((NX, NZ, 4, block, gcols), F32),
        acc_b=pltpu.VMEM((NY, NZ, 4, block, gcols), F32),
        acc_c=pltpu.VMEM((NZ, NY, 4, block, gcols), F32),
        sent_a=ring_buffer(NX, NZ),
        sent_b=ring_buffer(NY, NZ),
        sent_c=ring_buffer(NZ, NY),
        came_a=ring_buffer(NX, NZ),
        came_b=ring_buffer(NY, NZ),
        came_c=ring_buffer(NZ, NY),
        sent2_a=pieces(2, 3, NZ // 2),
        sent2_b=pieces(2, 3, NZ // 2),
        came2_a=pieces(2, 3, NZ // 2),
        came2_b=pieces(2, 3, NZ // 2),
        line=pltpu.VMEM((2, NZ, block, gcols), F32),
        sent3_a=pieces(NZ - 1),
        sent3_b=pieces(NZ - 1),
        came3_a=pieces(NZ - 1),
        came3_b=pieces(NZ - 1),
        sent_p=pieces(PLANE - 1),
        came_p=pieces(PLANE - 1),
        flat=pltpu.VMEM((PLANE * share, LANES), F32),
        parts=pltpu.VMEM((PLANE - 1, share, LANES), F32),
        pile=pltpu.VMEM((NZ, share, LANES), F32),
        whole=pltpu.VMEM((PLANE, share, LANES), BF16),
        in_sem=dma((8,)),
        tp_send=dma((2,)),
        tp_recv=dma((2,)),
        halo_send=dma,
        halo_recv=dma,
        ring_send=dma((GROUPS,)),
        ring_recv=dma((2 * (NX + NY + NZ) - 6,)),
        second_send=dma((2,)),
        second_recv=dma((2, 2)),
        third_send=dma((2,)),
        third_recv=dma((2,)),
        plane_send=dma,
        plane_recv=dma,
        gate_send=dma,
        gate_recv=dma,
        a_send=dma,
        a_recv=dma,
        b_send=dma,
        b_recv=dma,
        c_send=dma,
        c_recv=dma,
    )
    ins = ("cv_hbm", "cg_hbm", "co_hbm", "taps_hbm", "gain_hbm", "shift_hbm", "w_hbm", "og_hbm")
    outs = dict(
        gv=((rows, chan), BF16),
        gg=((rows, chan), BF16),
        taps_out=((ntaps, chan), F32),
        gain_out=((chan,), F32),
        shift_out=((chan,), F32),
        proj_out=((block, chan), F32),
    )
    results = pl.pallas_call(
        functools.partial(kernel, (*ins, *outs, *scratch)),
        out_shape=[pltpu.VMEM(*out) for out in outs.values()],
        in_specs=[pl.BlockSpec(memory_space=pltpu.HBM)] * 8,
        out_specs=[vmem] * len(outs),
        scratch_shapes=list(scratch.values()),
        compiler_params=pltpu.CompilerParams(
            collective_id=0, has_side_effects=True, vmem_limit_bytes=VMEM_LIMIT
        ),
    )(
        *[
            pltpu.with_memory_space_constraint(v, pltpu.HBM)
            for v in (
                conv_value, conv_gate, conv_out, conv_taps, norm_gain, norm_shift, proj_weight, out_grad,
            )
        ]
    )
    return pl.pallas_call(
        place,
        out_shape=[jax.ShapeDtypeStruct(*out) for out in outs.values()],
        in_specs=[vmem] * len(outs),
        out_specs=[hbm] * len(outs),
        scratch_shapes=[dma((len(outs),))],
        compiler_params=pltpu.CompilerParams(vmem_limit_bytes=1024 * 1024),
    )(*[pltpu.with_memory_space_constraint(v, pltpu.VMEM) for v in results])


def solution(mesh):
    in_specs = (
        P("sp", "tp"),
        P("sp", "tp"),
        P("sp", "tp"),
        P(None, "tp"),
        P("tp"),
        P("tp"),
        P(None, "tp"),
        P("sp", None),
    )
    out_specs = (P("sp", "tp"), P("sp", "tp"), P(None, "tp"), P("tp"), P("tp"), P("sp", "tp"))
    return jax.shard_map(local, mesh=mesh, in_specs=in_specs, out_specs=out_specs, check_vma=False)
```

```python
import functools
import types

import jax
import jax.numpy as jnp
from jax import lax
from jax.experimental import pallas as pl
from jax.experimental.pallas import tpu as pltpu
from jax.sharding import PartitionSpec as P

norm_eps = 1e-05
MESH = pl.DeviceIdType.MESH
F32 = jnp.float32
BF16 = jnp.bfloat16
LANES = 128
NX, NY, NZ = 4, 4, 8
PLANE = NX * NY
RING = (NX, NY, NZ)
GROUPS = 3
HALO = 32
VMEM_LIMIT = 48 * 1024 * 1024


def repeat(start, stop, body, unroll):
    assert (stop - start) % unroll == 0

    def step(i, carry):
        for u in range(unroll):
            body(start + i * unroll + u)
        return carry

    lax.fori_loop(0, (stop - start) // unroll, step, 0)


def kernel(names, *refs):
    r = types.SimpleNamespace(**dict(zip(names, refs)))
    rows, chan = r.co.shape
    width = r.og.shape[1]
    n = NX * NY * NZ
    block = width // n
    gcols = chan // GROUPS
    cblocks = chan // LANES
    ntaps = r.taps.shape[0]
    reach = ntaps - 1
    per = -(-(ntaps + 2) // 8) * 8
    share = r.parts.shape[2]
    chan_total = chan * 2
    me = lax.axis_index("sp")
    core = lax.axis_index("tp")
    x = lax.rem(me, NX)
    y = lax.rem(me // NX, NY)
    z = me // PLANE
    spot = lax.rem(me, PLANE)
    axes = ((x, NX, 1), (y, NY, NX), (z, NZ, PLANE))

    def along(axis, delta):
        c, size, stride = axis
        return me + (lax.rem(c + delta, size) - c) * stride

    def in_plane(i):
        return me - spot + lax.rem(spot + i, PLANE)

    def remote(src, dst, send, recv, device, to_core=None):
        return pltpu.make_async_remote_copy(
            src_ref=src, dst_ref=dst, send_sem=send, recv_sem=recv,
            device_id=(device, core if to_core is None else to_core), device_id_type=MESH,
        )

    loads = [
        pltpu.make_async_copy(src, dst, r.in_sem.at[i])
        for i, (src, dst) in enumerate(
            (
                (r.co_hbm, r.co), (r.og_hbm, r.og), (r.w_hbm, r.w), (r.cg_hbm, r.cg), (r.cv_hbm, r.cv),
                (r.taps_hbm, r.taps), (r.gain_hbm, r.gain), (r.shift_hbm, r.shift),
            )
        )
    ]
    loads[0].start()
    barrier = pltpu.get_barrier_semaphore()

    def greet(device, to_core):
        pl.semaphore_signal(barrier, inc=1, device_id=(device, to_core), device_id_type=MESH)

    greet(me, 1 - core)
    for i in range(1, NZ):
        greet(along(axes[2], i), core)
    for i in range(1, PLANE):
        greet(in_plane(i), core)
        greet(in_plane(i), 1 - core)
    has_prev = me > 0
    has_next = me < n - 1

    @pl.when(has_prev)
    def _():
        greet(me - 1, core)

    @pl.when(has_next)
    def _():
        greet(me + 1, core)

    friends = NZ + 2 * (PLANE - 1) + has_prev.astype(jnp.int32) + has_next.astype(jnp.int32)

    lane_low = lax.broadcasted_iota(jnp.int32, (1, LANES), 1) < LANES // 2
    nt = rows // LANES
    mid = LANES // 2

    def pack(dst):
        for t in range(nt):
            turned = r.st_a[t * LANES:(t + 1) * LANES, :].T
            dst[0, t:t + 1, :] = turned[:1, :]
            dst[1, t:t + 1, :] = turned[mid:mid + 1, :]

    def unpack(packed, dst):
        for t in range(nt):
            dst[t * LANES:(t + 1) * LANES, :] = jnp.broadcast_to(packed[t:t + 1, :], (LANES, LANES)).T

    def wide(v):
        return jnp.concatenate([v] * cblocks, axis=1)

    for i in (3, 4, 1, 2, 6, 7, 5):
        loads[i].start()
    loads[0].wait()

    def means(i):
        at = slice(i * 64, (i + 1) * 64)
        h = r.co[at, :].astype(F32)
        mean = jnp.sum(h, axis=1, keepdims=True) / chan
        r.st_b[at, :] = jnp.broadcast_to(mean, (64, LANES))

    def spreads(i):
        at = slice(i * 64, (i + 1) * 64)
        mean = r.st_b[at, :]
        m2 = jnp.zeros((64, LANES), F32)
        for c in range(cblocks):
            d = r.co[at, c * LANES:(c + 1) * LANES].astype(F32) - mean
            m2 = m2 + d * d
        r.st_a[at, :] = jnp.where(lane_low, mean, jnp.sum(m2, axis=1, keepdims=True))

    for i in range(rows // 64):
        means(i)
    for i in range(rows // 64):
        spreads(i)
    pack(r.pk_a)
    loads[3].wait()
    loads[4].wait()

    def gate_rows(i):
        at = pl.ds(pl.multiple_of(i * 32, 32), 32)
        value = r.cv[at, :].astype(F32)
        return (value * jax.nn.sigmoid(r.cg[at, :].astype(F32))).astype(BF16)

    r.gate_out[...] = gate_rows(rows // HALO - 1)

    def gate(i):
        at = pl.ds(pl.multiple_of(HALO + i * 32, 32), 32)
        gated = gate_rows(i).astype(F32)
        for c in range(cblocks):
            r.gx[c, at, :] = gated[:, c * LANES:(c + 1) * LANES]

    repeat(0, rows // 32, gate, 2)

    pl.semaphore_wait(barrier, friends)
    swap_a = remote(r.pk_a, r.pk_b, r.tp_send.at[0], r.tp_recv.at[0], me, 1 - core)
    swap_a.start()
    loads[1].wait()
    slab = width // NZ

    def transpose(c, carry):
        t = r.og[:, pl.ds(pl.multiple_of(c * slab, slab), slab)].T
        r.ogt[c] = t.reshape(NY, NX, block, rows)
        return carry

    lax.fori_loop(0, NZ, transpose, 0)
    gate_copy = remote(r.gate_out, r.gate_in, r.gate_send, r.gate_recv, lax.rem(me + 1, n))

    @pl.when(has_next)
    def _():
        gate_copy.start()

    loads[6].wait()
    loads[7].wait()
    gain = r.gain[...].reshape(1, chan)
    shift = r.shift[...].reshape(1, chan)
    swap_a.wait()
    gap = r.pk_a[0] - r.pk_b[0]
    variance = (r.pk_a[1] + r.pk_b[1] + gap * gap * (0.5 * chan)) / chan_total
    unpack(0.5 * (r.pk_a[0] + r.pk_b[0]), r.st_b)
    unpack(lax.rsqrt(variance + norm_eps), r.st_d)

    def norm(i):
        at = pl.ds(pl.multiple_of(i * 16, 16), 16)
        v = (r.co[at, :].astype(F32) - wide(r.st_b[at, :])) * wide(r.st_d[at, :])
        r.normed[at, :] = v
        t = v * gain + shift
        sig = jax.nn.sigmoid(t)
        r.active[at, :] = (t * sig).astype(BF16)
        r.dsilu[at, :] = sig * (1.0 + t * (1.0 - sig))

    repeat(0, rows // 16, norm, 4)

    acc = (r.acc_a, r.acc_b, r.acc_c)
    sent = (r.sent_a, r.sent_b, r.sent_c)
    came = (r.came_a, r.came_b, r.came_c)
    sent2 = (r.sent2_a, r.sent2_b)
    came2 = (r.came2_a, r.came2_b)
    sent3 = (r.sent3_a, r.sent3_b)
    came3 = (r.came3_a, r.came3_b)
    outer = (NZ, NZ, NY)
    second_axis = (1, 0)
    third_axis = (2, 2)
    first_recv = (0, 2 * NX - 2, 2 * NX + 2 * NY - 4)

    def slot(g, d, s, k):
        far = RING[g] // 2
        return d * (2 * far - 1) + (k - 1 if s == d else far + k - 1)

    def hop(g, d, s, k):
        i = slot(g, d, s, k)
        return remote(
            sent[g].at[i], came[g].at[i], r.ring_send.at[g], r.ring_recv.at[first_recv[g] + i],
            along(axes[g], 1 if d == 0 else RING[g] - 1),
        )

    def product(g, k):
        size = RING[g]
        far = size // 2
        half = outer[g] // 2
        at = lax.rem(axes[g][0] + k, size)
        lhs = r.ogt[:, :, at] if g == 0 else r.ogt[:, at] if g == 1 else r.ogt[at]
        lhs = lhs.reshape(-1, rows)
        out = jnp.dot(lhs, r.active[:, g * gcols:(g + 1) * gcols], preferred_element_type=F32)
        out = out.reshape(outer[g], 4, block, gcols)
        if k == far:
            for d in range(2):
                sent[g][slot(g, d, d, far)] = out[half * d:half * (d + 1)].astype(BF16)
        elif k in (far - 1, size - far + 1):
            d = 0 if k == far - 1 else 1
            s = 1 - d
            sent[g][slot(g, d, s, far - 1)] = out[half * s:half * (s + 1)].astype(BF16)
            acc[g][k, half * d:half * (d + 1)] = out[half * d:half * (d + 1)]
        else:
            acc[g][k] = out

    def launch(g, own):
        far = RING[g] // 2
        for d in range(2):
            if own:
                hop(g, d, 1 - d, far - 1).start()
            else:
                hop(g, d, d, far).start()

    def relay(g, d, s, k):
        size = RING[g]
        half = outer[g] // 2
        hop(g, d, s, k).wait_recv()
        at = k - 1 if d == 0 else (size - k + 1) % size
        total = acc[g][at, half * s:half * (s + 1)] + came[g][slot(g, d, s, k)].astype(F32)
        if k > 1:
            sent[g][slot(g, d, s, k - 1)] = total.astype(BF16)
            hop(g, d, s, k - 1).start()
        else:
            acc[g][at, half * s:half * (s + 1)] = total

    def start_plane():
        for i in range(1, PLANE):
            peer = lax.rem(spot + i, PLANE)
            r.sent_p[i - 1] = acc[2][0, peer // NX, lax.rem(peer, NX)].astype(BF16)
            remote(r.sent_p.at[i - 1], r.came_p.at[i - 1], r.plane_send, r.plane_recv, in_plane(i)).start()

    def finish_plane():
        remote(r.sent_p, r.came_p, r.plane_send, r.plane_recv, me).wait_recv()
        total = acc[2][0, y, x]
        for i in range(1, PLANE):
            total = total + r.came_p[i - 1].astype(F32)
        r.proj_out[:, 2 * gcols:] = total

    def start_second(g, s):
        half = outer[g] // 2
        c = axes[second_axis[g]][0]
        for i in range(1, 4):
            sent2[g][s, i - 1] = acc[g][0, half * s:half * (s + 1), lax.rem(c + i, 4)].astype(BF16)
            remote(
                sent2[g].at[s, i - 1], came2[g].at[s, i - 1],
                r.second_send.at[g], r.second_recv.at[g, s], along(axes[second_axis[g]], i),
            ).start()

    def finish_second(g, s):
        half = outer[g] // 2
        c = axes[second_axis[g]][0]
        remote(sent2[g].at[s], came2[g].at[s], r.second_send.at[g], r.second_recv.at[g, s], me).wait_recv()
        total = acc[g][0, half * s:half * (s + 1), c]
        for i in range(1, 4):
            total = total + came2[g][s, i - 1].astype(F32)
        r.line[g, half * s:half * (s + 1)] = total

    def start_third(g):
        c, size, _ = axes[third_axis[g]]
        for i in range(1, size):
            sent3[g][i - 1] = r.line[g, lax.rem(c + i, size)].astype(BF16)
            remote(
                sent3[g].at[i - 1], came3[g].at[i - 1],
                r.third_send.at[g], r.third_recv.at[g], along(axes[third_axis[g]], i),
            ).start()

    def finish_third(g):
        c, size, _ = axes[third_axis[g]]
        remote(sent3[g], came3[g], r.third_send.at[g], r.third_recv.at[g], me).wait_recv()
        total = r.line[g, c]
        for i in range(1, size):
            total = total + came3[g][i - 1].astype(F32)
        r.proj_out[:, g * gcols:(g + 1) * gcols] = total

    for g, k in ((2, 4), (0, 2), (1, 2)):
        product(g, k)
    for g in (2, 0, 1):
        launch(g, False)
    for g, k in ((2, 3), (2, 5), (0, 1), (0, 3), (1, 1), (1, 3)):
        product(g, k)
    for g in (2, 0, 1):
        launch(g, True)
    loads[2].wait()

    def act(i):
        cols = slice(i * gcols, (i + 1) * gcols)
        r.scaled[:, cols] = jnp.dot(r.og[...], r.w[:, cols], preferred_element_type=F32)

    def grads(i):
        cols = slice(i * gcols, (i + 1) * gcols)
        sums = [jnp.zeros((8, gcols), F32)] * 2
        for q in range(0, rows, 32):
            at = slice(q, q + 32)
            v = r.normed[at, cols]
            ng = r.scaled[at, cols] * r.dsilu[at, cols]
            sums = [
                sums[0] + jnp.sum((ng * v).reshape(4, 8, gcols), axis=0),
                sums[1] + jnp.sum(ng.reshape(4, 8, gcols), axis=0),
            ]
            s = ng * gain[:, cols]
            r.scaled[at, cols] = s
            for dst, t in ((r.st_a, s), (r.st_b, s * v)):
                t = t[:, :LANES] + t[:, LANES:]
                dst[at, :] = t if i == 0 else dst[at, :] + t
        for j in range(2):
            r.rowacc[j, :, cols] = sums[j]

    act(0)
    for i in range(1, GROUPS):
        act(i)
        grads(i - 1)
    grads(GROUPS - 1)

    for q in range(0, rows, 64):
        at = slice(q, q + 64)
        total = jnp.sum(r.st_a[at, :], axis=1, keepdims=True)
        dot = jnp.sum(r.st_b[at, :], axis=1, keepdims=True)
        r.st_a[at, :] = jnp.where(lane_low, total, dot)

    pack(r.pk_c)
    swap_b = remote(r.pk_c, r.pk_d, r.tp_send.at[1], r.tp_recv.at[1], me, 1 - core)
    swap_b.start()
    r.tapacc[...] = jnp.zeros_like(r.tapacc)
    loads[5].wait()
    for c in range(cblocks):
        r.tapf[c] = r.taps[:, c * LANES:(c + 1) * LANES].astype(F32)
    r.flat[...] = jnp.zeros_like(r.flat)
    for g, k in ((2, 2), (2, 6), (0, 0), (1, 0)):
        product(g, k)
    for d in range(2):
        relay(2, d, d, 4)
    swap_b.wait()
    unpack((r.pk_c[0] + r.pk_d[0]) / chan_total, r.st_a)
    unpack((r.pk_c[1] + r.pk_d[1]) / chan_total, r.st_b)

    def height_rows(i):
        at = pl.ds(pl.multiple_of(i * 32, 32), 32)
        hg = wide(r.st_d[at, :]) * (
            r.scaled[at, :] - wide(r.st_a[at, :]) - r.normed[at, :] * wide(r.st_b[at, :])
        )
        for c in range(cblocks):
            r.hgx[c, at, :] = hg[:, c * LANES:(c + 1) * LANES]
        return hg

    first = height_rows(0)
    for c in range(cblocks):
        r.halo_out[c] = first[:, c * LANES:(c + 1) * LANES].astype(BF16)
    halo_copy = remote(r.halo_out, r.halo_in, r.halo_send, r.halo_recv, lax.rem(me + n - 1, n))

    @pl.when(has_prev)
    def _():
        halo_copy.start()

    repeat(1, rows // 32, height_rows, 3)
    @pl.when(has_prev)
    def _():
        gate_copy.wait_recv()
        for c in range(cblocks):
            r.gx[c, :HALO, :] = r.gate_in[:, c * LANES:(c + 1) * LANES].astype(F32)

    @pl.when(jnp.logical_not(has_prev))
    def _():
        r.gx[:, :HALO, :] = jnp.zeros((cblocks, HALO, LANES), F32)

    tall = 128
    talls = rows // tall
    skip = HALO - reach

    def tap_block(i, carry):
        c = i // talls
        q = pl.multiple_of(lax.rem(i, talls) * tall, tall)
        hg = r.hgx[c, pl.ds(q, tall), :]
        for m in range(8):
            js = range(m, ntaps, 8)
            near = r.gx[c, pl.ds(q + skip + m, tall + 8 * (len(js) - 1)), :]
            for k, j in enumerate(js):
                both = near[8 * k:8 * k + tall] * hg
                r.tapacc[c, j] = r.tapacc[c, j] + jnp.sum(both.reshape(tall // 8, 8, LANES), axis=0)
        return carry

    early = 4
    lax.fori_loop(0, early, tap_block, 0)
    for g in range(2):
        for d in range(2):
            relay(g, d, d, 2)
    for d in range(2):
        relay(2, d, 1 - d, 3)
    lax.fori_loop(early, cblocks * talls, tap_block, 0)
    for c in range(cblocks):
        r.flat[c * per:c * per + ntaps, :] = jnp.sum(r.tapacc[c], axis=1)
        for j in range(2):
            r.flat[c * per + ntaps + j:c * per + ntaps + j + 1, :] = jnp.sum(
                r.rowacc[j, :, c * LANES:(c + 1) * LANES], axis=0, keepdims=True
            )

    r.packed[...] = r.flat[...].astype(BF16)

    def piece(i):
        return r.packed.at[pl.ds(pl.multiple_of(i * share, share), share)]

    for i in range(1, PLANE):
        remote(
            piece(lax.rem(spot + i, PLANE)), r.parts.at[core, i - 1], r.a_send, r.a_recv.at[core], in_plane(i), 1,
        ).start()

    @pl.when(core == 0)
    def _():
        remote(piece(spot), r.parts.at[0, PLANE - 1], r.a_send, r.a_recv.at[0], me, 1).start()

    @pl.when(core == 1)
    def _():
        r.parts[1, PLANE - 1] = piece(spot)[...]

    for d in range(2):
        relay(2, d, d, 3)
    for k in (1, 7, 0):
        product(2, k)
    for d in range(2):
        relay(2, d, 1 - d, 2)
    step = 64
    steps = rows // step

    def grad_block(i, carry):
        inner = i < cblocks * (steps - 1)
        c = jnp.where(inner, i // (steps - 1), i - cblocks * (steps - 1))
        q = pl.multiple_of(jnp.where(inner, lax.rem(i, steps - 1), steps - 1) * step, step)
        at = pl.ds(q, step)
        cols = pl.ds(pl.multiple_of(c * LANES, LANES), LANES)
        sig = jax.nn.sigmoid(r.cg[at, cols].astype(F32))
        value = r.cv[at, cols].astype(F32)
        total = jnp.zeros((step, LANES), F32)
        for m in range(8):
            ks = range(m, ntaps, 8)
            near = r.hgx[c, pl.ds(q + m, step + 8 * (len(ks) - 1)), :]
            for k, j in enumerate(ks):
                total = total + r.tapf[c, pl.ds(reach - j, 1), :] * near[8 * k:8 * k + step]
        r.gv[at, cols] = (total * sig).astype(BF16)
        r.gg[at, cols] = (total * value * sig * (1.0 - sig)).astype(BF16)
        return carry

    lax.fori_loop(0, 10, grad_block, 0)
    for g in range(2):
        for d in range(2):
            relay(g, d, 1 - d, 1)
    for g in range(2):
        for d in range(2):
            relay(g, d, d, 1)
    for g in range(2):
        for s in range(2):
            start_second(g, s)
    lax.fori_loop(10, 22, grad_block, 0)
    for d in range(2):
        relay(2, d, d, 2)
    lax.fori_loop(22, 28, grad_block, 0)
    theirs = r.parts.at[0]
    ours = r.parts.at[1, pl.ds(0, PLANE - 1)]
    nearby = r.pile.at[pl.ds(0, NZ - 1)]
    around = r.whole.at[pl.ds(0, PLANE - 1)]

    @pl.when(core == 1)
    def _():
        remote(theirs, theirs, r.a_send, r.a_recv.at[0], me).wait_recv()
        remote(ours, ours, r.a_send, r.a_recv.at[1], me).wait_recv()
        for f in range(2):
            mine = r.parts[f, 0].astype(F32)
            for i in range(1, PLANE):
                mine = mine + r.parts[f, i].astype(F32)
            r.pile[NZ - 1, f] = mine.astype(BF16)
        for i in range(1, NZ):
            remote(r.pile.at[NZ - 1], r.pile.at[i - 1], r.b_send, r.b_recv, along(axes[2], i)).start()

    lax.fori_loop(28, 38, grad_block, 0)
    for g in range(2):
        for s in range(2):
            finish_second(g, s)
        start_third(g)
    for d in range(2):
        relay(2, d, 1 - d, 1)
    for d in range(2):
        relay(2, d, d, 1)
    start_plane()

    @pl.when(core == 1)
    def _():
        remote(nearby, nearby, r.b_send, r.b_recv, me).wait_recv()
        mine = r.pile[lax.rem(z + NZ - 1, NZ)].astype(F32)
        for i in range(1, NZ):
            mine = mine + r.pile[lax.rem(z - i + 2 * NZ - 1, NZ)].astype(F32)
        r.final[...] = mine.astype(BF16)
        for to in range(2):
            for i in range(1, PLANE):
                remote(r.final.at[to], r.whole.at[i - 1], r.c_send, r.c_recv, in_plane(i), to).start()
        remote(r.final.at[0], r.whole.at[PLANE - 1], r.c_send, r.c_recv, me, 0).start()
        r.whole[PLANE - 1] = mine[1].astype(BF16)


    @pl.when(has_next)
    def _():
        halo_copy.wait_recv()
        r.hgx[:, rows:, :] = r.halo_in[...].astype(F32)

    @pl.when(jnp.logical_not(has_next))
    def _():
        r.hgx[:, rows:, :] = jnp.zeros((cblocks, HALO, LANES), F32)

    lax.fori_loop(38, cblocks * steps, grad_block, 0)
    finish_third(0)
    finish_third(1)

    @pl.when(core == 0)
    def _():
        remote(r.whole, r.whole, r.c_send, r.c_recv, me).wait_recv()

    @pl.when(core == 1)
    def _():
        remote(around, around, r.c_send, r.c_recv, me).wait_recv()

    gains, shifts = [], []
    for c in range(cblocks):
        cols = slice(c * LANES, (c + 1) * LANES)
        for m in range(0, per, 8):
            row = c * per + m
            seg = r.whole[lax.rem(spot - row // share + 2 * PLANE - 1, PLANE)].astype(F32)
            seg = seg[row % share:row % share + 8]
            for q in range(m, m + 8):
                if q == ntaps:
                    gains.append(seg[q - m:q - m + 1])
                elif q == ntaps + 1:
                    shifts.append(seg[q - m:q - m + 1])
            if m < ntaps:
                end = min(m + 8, ntaps)
                r.taps_out[m:end, cols] = seg[:end - m]
    r.gain_out[...] = jnp.concatenate(gains, axis=1).reshape(chan)
    r.shift_out[...] = jnp.concatenate(shifts, axis=1).reshape(chan)
    finish_plane()
    for g in range(GROUPS):
        remote(sent[g], came[g], r.ring_send.at[g], r.ring_recv.at[0], me).wait_send()
    for g in range(2):
        remote(sent2[g], came2[g], r.second_send.at[g], r.second_recv.at[g, 0], me).wait_send()
        remote(sent3[g], came3[g], r.third_send.at[g], r.third_recv.at[g], me).wait_send()
    remote(r.sent_p, r.came_p, r.plane_send, r.plane_recv, me).wait_send()

    @pl.when(core == 0)
    def _():
        remote(theirs, theirs, r.a_send, r.a_recv.at[0], me).wait_send()

    @pl.when(core == 1)
    def _():
        remote(ours, ours, r.a_send, r.a_recv.at[1], me).wait_send()
        remote(nearby, nearby, r.b_send, r.b_recv, me).wait_send()
        remote(r.whole, r.whole, r.c_send, r.c_recv, me).wait_send()
        remote(around, around, r.c_send, r.c_recv, me).wait_send()

    @pl.when(has_prev)
    def _():
        halo_copy.wait_send()

    @pl.when(has_next)
    def _():
        gate_copy.wait_send()


def place(*refs):
    arrays = (len(refs) - 1) // 2
    copies = [
        pltpu.make_async_copy(refs[i], refs[arrays + i], refs[-1].at[i]) for i in range(arrays)
    ]
    for copy in copies:
        copy.start()
    for copy in copies:
        copy.wait()


def local(conv_value, conv_gate, conv_out, conv_taps, norm_gain, norm_shift, proj_weight, out_grad):
    rows, chan = conv_value.shape
    ntaps = conv_taps.shape[0]
    width = out_grad.shape[1]
    n = lax.axis_size("sp")
    assert n == NX * NY * NZ and lax.axis_size("tp") == 2
    gcols = chan // GROUPS
    block = width // n
    cblocks = chan // LANES
    per = -(-(ntaps + 2) // 8) * 8
    share = -(-(-(-per * cblocks // PLANE)) // 16) * 16
    hbm = pl.BlockSpec(memory_space=pl.ANY)
    vmem = pl.BlockSpec(memory_space=pltpu.VMEM)
    dma = pltpu.SemaphoreType.DMA

    def ring_buffer(size, deep):
        return pltpu.VMEM((2 * size - 2, deep // 2, 4, block, gcols), BF16)

    def pieces(*lead):
        return pltpu.VMEM((*lead, block, gcols), BF16)

    scratch = dict(
        cv=pltpu.VMEM((rows, chan), BF16),
        cg=pltpu.VMEM((rows, chan), BF16),
        co=pltpu.VMEM((rows, chan), BF16),
        w=pltpu.VMEM((width, chan), BF16),
        og=pltpu.VMEM((rows, width), BF16),
        taps=pltpu.VMEM((ntaps, chan), BF16),
        gain=pltpu.VMEM((chan,), F32),
        shift=pltpu.VMEM((chan,), F32),
        ogt=pltpu.VMEM((NZ, NY, NX, block, rows), BF16),
        active=pltpu.VMEM((rows, chan), BF16),
        normed=pltpu.VMEM((rows, chan), F32),
        dsilu=pltpu.VMEM((rows, chan), F32),
        scaled=pltpu.VMEM((rows, chan), F32),
        hgx=pltpu.VMEM((cblocks, rows + HALO, LANES), F32),
        st_a=pltpu.VMEM((rows, LANES), F32),
        st_b=pltpu.VMEM((rows, LANES), F32),
        st_d=pltpu.VMEM((rows, LANES), F32),
        pk_a=pltpu.VMEM((2, rows // LANES, LANES), F32),
        pk_b=pltpu.VMEM((2, rows // LANES, LANES), F32),
        pk_c=pltpu.VMEM((2, rows // LANES, LANES), F32),
        pk_d=pltpu.VMEM((2, rows // LANES, LANES), F32),
        tapf=pltpu.VMEM((cblocks, ntaps, LANES), F32),
        tapacc=pltpu.VMEM((cblocks, ntaps, 8, LANES), F32),
        rowacc=pltpu.VMEM((2, 8, chan), F32),
        gx=pltpu.VMEM((cblocks, HALO + rows, LANES), F32),
        gate_out=pltpu.VMEM((HALO, chan), BF16),
        gate_in=pltpu.VMEM((HALO, chan), BF16),
        halo_out=pltpu.VMEM((cblocks, HALO, LANES), BF16),
        halo_in=pltpu.VMEM((cblocks, HALO, LANES), BF16),
        acc_a=pltpu.VMEM((NX, NZ, 4, block, gcols), F32),
        acc_b=pltpu.VMEM((NY, NZ, 4, block, gcols), F32),
        acc_c=pltpu.VMEM((NZ, NY, 4, block, gcols), F32),
        sent_a=ring_buffer(NX, NZ),
        sent_b=ring_buffer(NY, NZ),
        sent_c=ring_buffer(NZ, NY),
        came_a=ring_buffer(NX, NZ),
        came_b=ring_buffer(NY, NZ),
        came_c=ring_buffer(NZ, NY),
        sent2_a=pieces(2, 3, NZ // 2),
        sent2_b=pieces(2, 3, NZ // 2),
        came2_a=pieces(2, 3, NZ // 2),
        came2_b=pieces(2, 3, NZ // 2),
        line=pltpu.VMEM((2, NZ, block, gcols), F32),
        sent3_a=pieces(NZ - 1),
        sent3_b=pieces(NZ - 1),
        came3_a=pieces(NZ - 1),
        came3_b=pieces(NZ - 1),
        sent_p=pieces(PLANE - 1),
        came_p=pieces(PLANE - 1),
        flat=pltpu.VMEM((PLANE * share, LANES), F32),
        packed=pltpu.VMEM((PLANE * share, LANES), BF16),
        parts=pltpu.VMEM((2, PLANE, share, LANES), BF16),
        pile=pltpu.VMEM((NZ, 2, share, LANES), BF16),
        final=pltpu.VMEM((2, share, LANES), BF16),
        whole=pltpu.VMEM((PLANE, share, LANES), BF16),
        in_sem=dma((8,)),
        tp_send=dma((2,)),
        tp_recv=dma((2,)),
        halo_send=dma,
        halo_recv=dma,
        ring_send=dma((GROUPS,)),
        ring_recv=dma((2 * (NX + NY + NZ) - 6,)),
        second_send=dma((2,)),
        second_recv=dma((2, 2)),
        third_send=dma((2,)),
        third_recv=dma((2,)),
        plane_send=dma,
        plane_recv=dma,
        gate_send=dma,
        gate_recv=dma,
        a_send=dma,
        a_recv=dma((2,)),
        b_send=dma,
        b_recv=dma,
        c_send=dma,
        c_recv=dma,
    )
    ins = ("cv_hbm", "cg_hbm", "co_hbm", "taps_hbm", "gain_hbm", "shift_hbm", "w_hbm", "og_hbm")
    outs = dict(
        gv=((rows, chan), BF16),
        gg=((rows, chan), BF16),
        taps_out=((ntaps, chan), F32),
        gain_out=((chan,), F32),
        shift_out=((chan,), F32),
        proj_out=((block, chan), F32),
    )
    results = pl.pallas_call(
        functools.partial(kernel, (*ins, *outs, *scratch)),
        out_shape=[pltpu.VMEM(*out) for out in outs.values()],
        in_specs=[pl.BlockSpec(memory_space=pltpu.HBM)] * 8,
        out_specs=[vmem] * len(outs),
        scratch_shapes=list(scratch.values()),
        compiler_params=pltpu.CompilerParams(
            collective_id=0, has_side_effects=True, vmem_limit_bytes=VMEM_LIMIT
        ),
    )(
        *[
            pltpu.with_memory_space_constraint(v, pltpu.HBM)
            for v in (
                conv_value, conv_gate, conv_out, conv_taps, norm_gain, norm_shift, proj_weight, out_grad,
            )
        ]
    )
    return pl.pallas_call(
        place,
        out_shape=[jax.ShapeDtypeStruct(*out) for out in outs.values()],
        in_specs=[vmem] * len(outs),
        out_specs=[hbm] * len(outs),
        scratch_shapes=[dma((len(outs),))],
        compiler_params=pltpu.CompilerParams(vmem_limit_bytes=1024 * 1024),
    )(*[pltpu.with_memory_space_constraint(v, pltpu.VMEM) for v in results])


def solution(mesh):
    in_specs = (
        P("sp", "tp"),
        P("sp", "tp"),
        P("sp", "tp"),
        P(None, "tp"),
        P("tp"),
        P("tp"),
        P(None, "tp"),
        P("sp", None),
    )
    out_specs = (P("sp", "tp"), P("sp", "tp"), P(None, "tp"), P("tp"), P("tp"), P("sp", "tp"))
    return jax.shard_map(local, mesh=mesh, in_specs=in_specs, out_specs=out_specs, check_vma=False)
```

```python
import functools
import types

import jax
import jax.numpy as jnp
from jax import lax
from jax.experimental import pallas as pl
from jax.experimental.pallas import tpu as pltpu
from jax.sharding import PartitionSpec as P

norm_eps = 1e-05
MESH = pl.DeviceIdType.MESH
F32 = jnp.float32
BF16 = jnp.bfloat16
LANES = 128
NX, NY, NZ = 4, 4, 8
PLANE = NX * NY
RING = (NX, NY, NZ)
GROUPS = 3
HALO = 32
VMEM_LIMIT = 48 * 1024 * 1024


def repeat(start, stop, body, unroll):
    assert (stop - start) % unroll == 0

    def step(i, carry):
        for u in range(unroll):
            body(start + i * unroll + u)
        return carry

    lax.fori_loop(0, (stop - start) // unroll, step, 0)


def kernel(names, *refs):
    r = types.SimpleNamespace(**dict(zip(names, refs)))
    rows, chan = r.co.shape
    width = r.og.shape[1]
    n = NX * NY * NZ
    block = width // n
    gcols = chan // GROUPS
    cblocks = chan // LANES
    ntaps = r.taps.shape[0]
    reach = ntaps - 1
    per = -(-(ntaps + 2) // 8) * 8
    share = r.parts.shape[2]
    chan_total = chan * 2
    me = lax.axis_index("sp")
    core = lax.axis_index("tp")
    x = lax.rem(me, NX)
    y = lax.rem(me // NX, NY)
    z = me // PLANE
    spot = lax.rem(me, PLANE)
    axes = ((x, NX, 1), (y, NY, NX), (z, NZ, PLANE))

    def along(axis, delta):
        c, size, stride = axis
        return me + (lax.rem(c + delta, size) - c) * stride

    def in_plane(i):
        return me - spot + lax.rem(spot + i, PLANE)

    def remote(src, dst, send, recv, device, to_core=None):
        return pltpu.make_async_remote_copy(
            src_ref=src, dst_ref=dst, send_sem=send, recv_sem=recv,
            device_id=(device, core if to_core is None else to_core), device_id_type=MESH,
        )

    loads = [
        pltpu.make_async_copy(src, dst, r.in_sem.at[i])
        for i, (src, dst) in enumerate(
            (
                (r.co_hbm, r.co), (r.og_hbm, r.og), (r.w_hbm, r.w), (r.cg_hbm, r.cg), (r.cv_hbm, r.cv),
                (r.taps_hbm, r.taps), (r.gain_hbm, r.gain), (r.shift_hbm, r.shift),
            )
        )
    ]
    loads[0].start()
    barrier = pltpu.get_barrier_semaphore()

    def greet(device, to_core):
        pl.semaphore_signal(barrier, inc=1, device_id=(device, to_core), device_id_type=MESH)

    greet(me, 1 - core)
    for i in range(1, NZ):
        greet(along(axes[2], i), core)
    for i in range(1, PLANE):
        greet(in_plane(i), core)
        greet(in_plane(i), 1 - core)
    has_prev = me > 0
    has_next = me < n - 1

    @pl.when(has_prev)
    def _():
        greet(me - 1, core)

    @pl.when(has_next)
    def _():
        greet(me + 1, core)

    friends = NZ + 2 * (PLANE - 1) + has_prev.astype(jnp.int32) + has_next.astype(jnp.int32)

    lane_low = lax.broadcasted_iota(jnp.int32, (1, LANES), 1) < LANES // 2
    nt = rows // LANES
    mid = LANES // 2

    def pack(dst):
        for t in range(nt):
            turned = r.st_a[t * LANES:(t + 1) * LANES, :].T
            dst[0, t:t + 1, :] = turned[:1, :]
            dst[1, t:t + 1, :] = turned[mid:mid + 1, :]

    def unpack(packed, dst):
        for t in range(nt):
            dst[t * LANES:(t + 1) * LANES, :] = jnp.broadcast_to(packed[t:t + 1, :], (LANES, LANES)).T

    def wide(v):
        return jnp.concatenate([v] * cblocks, axis=1)

    for i in (3, 4, 1, 2, 6, 7, 5):
        loads[i].start()
    loads[0].wait()

    def means(i):
        at = slice(i * 64, (i + 1) * 64)
        h = r.co[at, :].astype(F32)
        mean = jnp.sum(h, axis=1, keepdims=True) / chan
        r.st_b[at, :] = jnp.broadcast_to(mean, (64, LANES))

    def spreads(i):
        at = slice(i * 64, (i + 1) * 64)
        mean = r.st_b[at, :]
        m2 = jnp.zeros((64, LANES), F32)
        for c in range(cblocks):
            d = r.co[at, c * LANES:(c + 1) * LANES].astype(F32) - mean
            m2 = m2 + d * d
        r.st_a[at, :] = jnp.where(lane_low, mean, jnp.sum(m2, axis=1, keepdims=True))

    for i in range(rows // 64):
        means(i)
    for i in range(rows // 64):
        spreads(i)
    pack(r.pk_a)
    loads[3].wait()
    loads[4].wait()

    def gate_rows(i):
        at = pl.ds(pl.multiple_of(i * 32, 32), 32)
        value = r.cv[at, :].astype(F32)
        return (value * jax.nn.sigmoid(r.cg[at, :].astype(F32))).astype(BF16)

    r.gate_out[...] = gate_rows(rows // HALO - 1)

    def gate(i):
        at = pl.ds(pl.multiple_of(HALO + i * 32, 32), 32)
        gated = gate_rows(i).astype(F32)
        for c in range(cblocks):
            r.gx[c, at, :] = gated[:, c * LANES:(c + 1) * LANES]

    repeat(0, rows // 32, gate, 2)

    loads[1].wait()
    slab = width // NZ

    def transpose(c, carry):
        t = r.og[:, pl.ds(pl.multiple_of(c * slab, slab), slab)].T
        r.ogt[c] = t.reshape(NY, NX, block, rows)
        return carry

    lax.fori_loop(0, NZ, transpose, 0)
    pl.semaphore_wait(barrier, friends)
    swap_a = remote(r.pk_a, r.pk_b, r.tp_send.at[0], r.tp_recv.at[0], me, 1 - core)
    swap_a.start()
    gate_copy = remote(r.gate_out, r.gate_in, r.gate_send, r.gate_recv, lax.rem(me + 1, n))

    @pl.when(has_next)
    def _():
        gate_copy.start()

    loads[6].wait()
    loads[7].wait()
    gain = r.gain[...].reshape(1, chan)
    shift = r.shift[...].reshape(1, chan)
    loads[2].wait()
    def act(i):
        cols = slice(i * gcols, (i + 1) * gcols)
        r.scaled[:, cols] = jnp.dot(r.og[...], r.w[:, cols], preferred_element_type=F32)

    act(0)
    swap_a.wait()
    gap = r.pk_a[0] - r.pk_b[0]
    variance = (r.pk_a[1] + r.pk_b[1] + gap * gap * (0.5 * chan)) / chan_total
    unpack(0.5 * (r.pk_a[0] + r.pk_b[0]), r.st_b)
    unpack(lax.rsqrt(variance + norm_eps), r.st_d)

    def norm(i):
        at = pl.ds(pl.multiple_of(i * 16, 16), 16)
        v = (r.co[at, :].astype(F32) - wide(r.st_b[at, :])) * wide(r.st_d[at, :])
        r.normed[at, :] = v
        t = v * gain + shift
        sig = jax.nn.sigmoid(t)
        r.active[at, :] = (t * sig).astype(BF16)
        r.dsilu[at, :] = sig * (1.0 + t * (1.0 - sig))

    repeat(0, rows // 16, norm, 4)

    acc = (r.acc_a, r.acc_b, r.acc_c)
    sent = (r.sent_a, r.sent_b, r.sent_c)
    came = (r.came_a, r.came_b, r.came_c)
    sent2 = (r.sent2_a, r.sent2_b)
    came2 = (r.came2_a, r.came2_b)
    sent3 = (r.sent3_a, r.sent3_b)
    came3 = (r.came3_a, r.came3_b)
    outer = (NZ, NZ, NY)
    second_axis = (1, 0)
    third_axis = (2, 2)
    first_recv = (0, 2 * NX - 2, 2 * NX + 2 * NY - 4)

    def slot(g, d, s, k):
        far = RING[g] // 2
        return d * (2 * far - 1) + (k - 1 if s == d else far + k - 1)

    def hop(g, d, s, k):
        i = slot(g, d, s, k)
        return remote(
            sent[g].at[i], came[g].at[i], r.ring_send.at[g], r.ring_recv.at[first_recv[g] + i],
            along(axes[g], 1 if d == 0 else RING[g] - 1),
        )

    def product(g, k):
        size = RING[g]
        far = size // 2
        half = outer[g] // 2
        at = lax.rem(axes[g][0] + k, size)
        lhs = r.ogt[:, :, at] if g == 0 else r.ogt[:, at] if g == 1 else r.ogt[at]
        lhs = lhs.reshape(-1, rows)
        out = jnp.dot(lhs, r.active[:, g * gcols:(g + 1) * gcols], preferred_element_type=F32)
        out = out.reshape(outer[g], 4, block, gcols)
        if k == far:
            for d in range(2):
                sent[g][slot(g, d, d, far)] = out[half * d:half * (d + 1)].astype(BF16)
        elif k in (far - 1, size - far + 1):
            d = 0 if k == far - 1 else 1
            s = 1 - d
            sent[g][slot(g, d, s, far - 1)] = out[half * s:half * (s + 1)].astype(BF16)
            acc[g][k, half * d:half * (d + 1)] = out[half * d:half * (d + 1)]
        else:
            acc[g][k] = out

    def launch(g, own):
        far = RING[g] // 2
        for d in range(2):
            if own:
                hop(g, d, 1 - d, far - 1).start()
            else:
                hop(g, d, d, far).start()

    def relay(g, d, s, k):
        size = RING[g]
        half = outer[g] // 2
        hop(g, d, s, k).wait_recv()
        at = k - 1 if d == 0 else (size - k + 1) % size
        total = acc[g][at, half * s:half * (s + 1)] + came[g][slot(g, d, s, k)].astype(F32)
        if k > 1:
            sent[g][slot(g, d, s, k - 1)] = total.astype(BF16)
            hop(g, d, s, k - 1).start()
        else:
            acc[g][at, half * s:half * (s + 1)] = total

    def start_plane():
        for i in range(1, PLANE):
            peer = lax.rem(spot + i, PLANE)
            r.sent_p[i - 1] = acc[2][0, peer // NX, lax.rem(peer, NX)].astype(BF16)
            remote(r.sent_p.at[i - 1], r.came_p.at[i - 1], r.plane_send, r.plane_recv, in_plane(i)).start()

    def finish_plane():
        remote(r.sent_p, r.came_p, r.plane_send, r.plane_recv, me).wait_recv()
        total = acc[2][0, y, x]
        for i in range(1, PLANE):
            total = total + r.came_p[i - 1].astype(F32)
        r.proj_out[:, 2 * gcols:] = total

    def start_second(g, s):
        half = outer[g] // 2
        c = axes[second_axis[g]][0]
        for i in range(1, 4):
            sent2[g][s, i - 1] = acc[g][0, half * s:half * (s + 1), lax.rem(c + i, 4)].astype(BF16)
            remote(
                sent2[g].at[s, i - 1], came2[g].at[s, i - 1],
                r.second_send.at[g], r.second_recv.at[g, s], along(axes[second_axis[g]], i),
            ).start()

    def finish_second(g, s):
        half = outer[g] // 2
        c = axes[second_axis[g]][0]
        remote(sent2[g].at[s], came2[g].at[s], r.second_send.at[g], r.second_recv.at[g, s], me).wait_recv()
        total = acc[g][0, half * s:half * (s + 1), c]
        for i in range(1, 4):
            total = total + came2[g][s, i - 1].astype(F32)
        r.line[g, half * s:half * (s + 1)] = total

    def start_third(g):
        c, size, _ = axes[third_axis[g]]
        for i in range(1, size):
            sent3[g][i - 1] = r.line[g, lax.rem(c + i, size)].astype(BF16)
            remote(
                sent3[g].at[i - 1], came3[g].at[i - 1],
                r.third_send.at[g], r.third_recv.at[g], along(axes[third_axis[g]], i),
            ).start()

    def finish_third(g):
        c, size, _ = axes[third_axis[g]]
        remote(sent3[g], came3[g], r.third_send.at[g], r.third_recv.at[g], me).wait_recv()
        total = r.line[g, c]
        for i in range(1, size):
            total = total + came3[g][i - 1].astype(F32)
        r.proj_out[:, g * gcols:(g + 1) * gcols] = total

    for g, k in ((2, 4), (0, 2), (1, 2)):
        product(g, k)
    for g in (2, 0, 1):
        launch(g, False)
    for g, k in ((2, 3), (2, 5), (0, 1), (0, 3), (1, 1), (1, 3)):
        product(g, k)
    for g in (2, 0, 1):
        launch(g, True)

    def grads(i):
        cols = slice(i * gcols, (i + 1) * gcols)
        sums = [jnp.zeros((8, gcols), F32)] * 2
        for q in range(0, rows, 32):
            at = slice(q, q + 32)
            v = r.normed[at, cols]
            ng = r.scaled[at, cols] * r.dsilu[at, cols]
            sums = [
                sums[0] + jnp.sum((ng * v).reshape(4, 8, gcols), axis=0),
                sums[1] + jnp.sum(ng.reshape(4, 8, gcols), axis=0),
            ]
            s = ng * gain[:, cols]
            r.scaled[at, cols] = s
            for dst, t in ((r.st_a, s), (r.st_b, s * v)):
                t = t[:, :LANES] + t[:, LANES:]
                dst[at, :] = t if i == 0 else dst[at, :] + t
        for j in range(2):
            r.rowacc[j, :, cols] = sums[j]

    for i in range(1, GROUPS):
        act(i)
        grads(i - 1)
    grads(GROUPS - 1)

    for q in range(0, rows, 64):
        at = slice(q, q + 64)
        total = jnp.sum(r.st_a[at, :], axis=1, keepdims=True)
        dot = jnp.sum(r.st_b[at, :], axis=1, keepdims=True)
        r.st_a[at, :] = jnp.where(lane_low, total, dot)

    pack(r.pk_c)
    swap_b = remote(r.pk_c, r.pk_d, r.tp_send.at[1], r.tp_recv.at[1], me, 1 - core)
    swap_b.start()
    r.tapacc[...] = jnp.zeros_like(r.tapacc)
    loads[5].wait()
    for c in range(cblocks):
        r.tapf[c] = r.taps[:, c * LANES:(c + 1) * LANES].astype(F32)
    r.flat[...] = jnp.zeros_like(r.flat)
    for g, k in ((2, 2), (2, 6), (0, 0)):
        product(g, k)
    for d in range(2):
        relay(2, d, d, 4)
    product(1, 0)
    swap_b.wait()
    unpack((r.pk_c[0] + r.pk_d[0]) / chan_total, r.st_a)
    unpack((r.pk_c[1] + r.pk_d[1]) / chan_total, r.st_b)

    def height_rows(i):
        at = pl.ds(pl.multiple_of(i * 32, 32), 32)
        hg = wide(r.st_d[at, :]) * (
            r.scaled[at, :] - wide(r.st_a[at, :]) - r.normed[at, :] * wide(r.st_b[at, :])
        )
        for c in range(cblocks):
            r.hgx[c, at, :] = hg[:, c * LANES:(c + 1) * LANES]
        return hg

    first = height_rows(0)
    for c in range(cblocks):
        r.halo_out[c] = first[:, c * LANES:(c + 1) * LANES].astype(BF16)
    halo_copy = remote(r.halo_out, r.halo_in, r.halo_send, r.halo_recv, lax.rem(me + n - 1, n))

    @pl.when(has_prev)
    def _():
        halo_copy.start()

    repeat(1, rows // 32, height_rows, 3)
    @pl.when(has_prev)
    def _():
        gate_copy.wait_recv()
        for c in range(cblocks):
            r.gx[c, :HALO, :] = r.gate_in[:, c * LANES:(c + 1) * LANES].astype(F32)

    @pl.when(jnp.logical_not(has_prev))
    def _():
        r.gx[:, :HALO, :] = jnp.zeros((cblocks, HALO, LANES), F32)

    tall = 128
    talls = rows // tall
    skip = HALO - reach

    def tap_block(i, carry):
        c = i // talls
        q = pl.multiple_of(lax.rem(i, talls) * tall, tall)
        hg = r.hgx[c, pl.ds(q, tall), :]
        for m in range(8):
            js = range(m, ntaps, 8)
            near = r.gx[c, pl.ds(q + skip + m, tall + 8 * (len(js) - 1)), :]
            for k, j in enumerate(js):
                both = near[8 * k:8 * k + tall] * hg
                r.tapacc[c, j] = r.tapacc[c, j] + jnp.sum(both.reshape(tall // 8, 8, LANES), axis=0)
        return carry

    early = 4
    lax.fori_loop(0, early, tap_block, 0)
    for g in range(2):
        for d in range(2):
            relay(g, d, d, 2)
    for d in range(2):
        relay(2, d, 1 - d, 3)
    late = 20
    lax.fori_loop(early, late, tap_block, 0)
    for d in range(2):
        relay(2, d, d, 3)
    lax.fori_loop(late, cblocks * talls, tap_block, 0)
    for c in range(cblocks):
        r.flat[c * per:c * per + ntaps, :] = jnp.sum(r.tapacc[c], axis=1)
        for j in range(2):
            r.flat[c * per + ntaps + j:c * per + ntaps + j + 1, :] = jnp.sum(
                r.rowacc[j, :, c * LANES:(c + 1) * LANES], axis=0, keepdims=True
            )

    r.packed[...] = r.flat[...].astype(BF16)

    def piece(i):
        return r.packed.at[pl.ds(pl.multiple_of(i * share, share), share)]

    for i in range(1, PLANE):
        remote(
            piece(lax.rem(spot + i, PLANE)), r.parts.at[core, i - 1], r.a_send, r.a_recv.at[core], in_plane(i), 1,
        ).start()

    @pl.when(core == 0)
    def _():
        remote(piece(spot), r.parts.at[0, PLANE - 1], r.a_send, r.a_recv.at[0], me, 1).start()

    @pl.when(core == 1)
    def _():
        r.parts[1, PLANE - 1] = piece(spot)[...]

    for k in (1, 7, 0):
        product(2, k)
    for d in range(2):
        relay(2, d, 1 - d, 2)
    step = 64
    steps = rows // step

    def grad_block(i, carry):
        inner = i < cblocks * (steps - 1)
        c = jnp.where(inner, i // (steps - 1), i - cblocks * (steps - 1))
        q = pl.multiple_of(jnp.where(inner, lax.rem(i, steps - 1), steps - 1) * step, step)
        at = pl.ds(q, step)
        cols = pl.ds(pl.multiple_of(c * LANES, LANES), LANES)
        sig = jax.nn.sigmoid(r.cg[at, cols].astype(F32))
        value = r.cv[at, cols].astype(F32)
        total = jnp.zeros((step, LANES), F32)
        for m in range(8):
            ks = range(m, ntaps, 8)
            near = r.hgx[c, pl.ds(q + m, step + 8 * (len(ks) - 1)), :]
            for k, j in enumerate(ks):
                total = total + r.tapf[c, pl.ds(reach - j, 1), :] * near[8 * k:8 * k + step]
        r.gv[at, cols] = (total * sig).astype(BF16)
        r.gg[at, cols] = (total * value * sig * (1.0 - sig)).astype(BF16)
        return carry

    lax.fori_loop(0, 10, grad_block, 0)
    for g in range(2):
        for d in range(2):
            relay(g, d, 1 - d, 1)
    for g in range(2):
        for d in range(2):
            relay(g, d, d, 1)
    for g in range(2):
        for s in range(2):
            start_second(g, s)
    lax.fori_loop(10, 20, grad_block, 0)
    for d in range(2):
        relay(2, d, d, 2)
    lax.fori_loop(20, 28, grad_block, 0)
    theirs = r.parts.at[0]
    ours = r.parts.at[1, pl.ds(0, PLANE - 1)]
    nearby = r.pile.at[pl.ds(0, NZ - 1)]
    around = r.whole.at[pl.ds(0, PLANE - 1)]

    @pl.when(core == 1)
    def _():
        remote(theirs, theirs, r.a_send, r.a_recv.at[0], me).wait_recv()
        remote(ours, ours, r.a_send, r.a_recv.at[1], me).wait_recv()
        for f in range(2):
            mine = r.parts[f, 0].astype(F32)
            for i in range(1, PLANE):
                mine = mine + r.parts[f, i].astype(F32)
            r.pile[NZ - 1, f] = mine.astype(BF16)
        for q in range(NZ):

            @pl.when(z != q)
            def _(q=q):
                remote(
                    r.pile.at[NZ - 1], r.pile.at[lax.rem(q - z + 2 * NZ - 1, NZ)], r.b_send, r.b_recv, q * PLANE + spot,
                ).start()

    lax.fori_loop(28, 38, grad_block, 0)
    for g in range(2):
        for s in range(2):
            finish_second(g, s)
        start_third(g)
    for d in range(2):
        relay(2, d, 1 - d, 1)
    for d in range(2):
        relay(2, d, d, 1)
    start_plane()

    @pl.when(core == 1)
    def _():
        remote(nearby, nearby, r.b_send, r.b_recv, me).wait_recv()
        mine = r.pile[lax.rem(z + NZ - 1, NZ)].astype(F32)
        for i in range(1, NZ):
            mine = mine + r.pile[lax.rem(z - i + 2 * NZ - 1, NZ)].astype(F32)
        r.final[...] = mine.astype(BF16)
        for q in range(PLANE):
            goes = r.whole.at[lax.rem(q - spot + 2 * PLANE - 1, PLANE)]

            @pl.when(spot != q)
            def _(q=q, goes=goes):
                remote(r.final.at[1], goes, r.c_send, r.c_recv, me - spot + q, 1).start()

            remote(r.final.at[0], goes, r.c_send, r.c_recv, me - spot + q, 0).start()

        r.whole[PLANE - 1] = mine[1].astype(BF16)


    @pl.when(has_next)
    def _():
        halo_copy.wait_recv()
        r.hgx[:, rows:, :] = r.halo_in[...].astype(F32)

    @pl.when(jnp.logical_not(has_next))
    def _():
        r.hgx[:, rows:, :] = jnp.zeros((cblocks, HALO, LANES), F32)

    lax.fori_loop(38, cblocks * steps, grad_block, 0)
    finish_third(0)
    finish_third(1)

    @pl.when(core == 0)
    def _():
        remote(r.whole, r.whole, r.c_send, r.c_recv, me).wait_recv()

    @pl.when(core == 1)
    def _():
        remote(around, around, r.c_send, r.c_recv, me).wait_recv()

    gains, shifts = [], []
    for c in range(cblocks):
        cols = slice(c * LANES, (c + 1) * LANES)
        for m in range(0, per, 8):
            row = c * per + m
            seg = r.whole[lax.rem(spot - row // share + 2 * PLANE - 1, PLANE)].astype(F32)
            seg = seg[row % share:row % share + 8]
            for q in range(m, m + 8):
                if q == ntaps:
                    gains.append(seg[q - m:q - m + 1])
                elif q == ntaps + 1:
                    shifts.append(seg[q - m:q - m + 1])
            if m < ntaps:
                end = min(m + 8, ntaps)
                r.taps_out[m:end, cols] = seg[:end - m]
    r.gain_out[...] = jnp.concatenate(gains, axis=1).reshape(chan)
    r.shift_out[...] = jnp.concatenate(shifts, axis=1).reshape(chan)
    finish_plane()
    for g in range(GROUPS):
        remote(sent[g], came[g], r.ring_send.at[g], r.ring_recv.at[0], me).wait_send()
    for g in range(2):
        remote(sent2[g], came2[g], r.second_send.at[g], r.second_recv.at[g, 0], me).wait_send()
        remote(sent3[g], came3[g], r.third_send.at[g], r.third_recv.at[g], me).wait_send()
    remote(r.sent_p, r.came_p, r.plane_send, r.plane_recv, me).wait_send()

    @pl.when(core == 0)
    def _():
        remote(theirs, theirs, r.a_send, r.a_recv.at[0], me).wait_send()

    @pl.when(core == 1)
    def _():
        remote(ours, ours, r.a_send, r.a_recv.at[1], me).wait_send()
        remote(nearby, nearby, r.b_send, r.b_recv, me).wait_send()
        remote(r.whole, r.whole, r.c_send, r.c_recv, me).wait_send()
        remote(around, around, r.c_send, r.c_recv, me).wait_send()

    @pl.when(has_prev)
    def _():
        halo_copy.wait_send()

    @pl.when(has_next)
    def _():
        gate_copy.wait_send()


def place(*refs):
    arrays = (len(refs) - 1) // 2
    copies = [
        pltpu.make_async_copy(refs[i], refs[arrays + i], refs[-1].at[i]) for i in range(arrays)
    ]
    for copy in copies:
        copy.start()
    for copy in copies:
        copy.wait()


def local(conv_value, conv_gate, conv_out, conv_taps, norm_gain, norm_shift, proj_weight, out_grad):
    rows, chan = conv_value.shape
    ntaps = conv_taps.shape[0]
    width = out_grad.shape[1]
    n = lax.axis_size("sp")
    assert n == NX * NY * NZ and lax.axis_size("tp") == 2
    gcols = chan // GROUPS
    block = width // n
    cblocks = chan // LANES
    per = -(-(ntaps + 2) // 8) * 8
    share = -(-(-(-per * cblocks // PLANE)) // 16) * 16
    hbm = pl.BlockSpec(memory_space=pl.ANY)
    vmem = pl.BlockSpec(memory_space=pltpu.VMEM)
    dma = pltpu.SemaphoreType.DMA

    def ring_buffer(size, deep):
        return pltpu.VMEM((2 * size - 2, deep // 2, 4, block, gcols), BF16)

    def pieces(*lead):
        return pltpu.VMEM((*lead, block, gcols), BF16)

    scratch = dict(
        cv=pltpu.VMEM((rows, chan), BF16),
        cg=pltpu.VMEM((rows, chan), BF16),
        co=pltpu.VMEM((rows, chan), BF16),
        w=pltpu.VMEM((width, chan), BF16),
        og=pltpu.VMEM((rows, width), BF16),
        taps=pltpu.VMEM((ntaps, chan), BF16),
        gain=pltpu.VMEM((chan,), F32),
        shift=pltpu.VMEM((chan,), F32),
        ogt=pltpu.VMEM((NZ, NY, NX, block, rows), BF16),
        active=pltpu.VMEM((rows, chan), BF16),
        normed=pltpu.VMEM((rows, chan), F32),
        dsilu=pltpu.VMEM((rows, chan), F32),
        scaled=pltpu.VMEM((rows, chan), F32),
        hgx=pltpu.VMEM((cblocks, rows + HALO, LANES), F32),
        st_a=pltpu.VMEM((rows, LANES), F32),
        st_b=pltpu.VMEM((rows, LANES), F32),
        st_d=pltpu.VMEM((rows, LANES), F32),
        pk_a=pltpu.VMEM((2, rows // LANES, LANES), F32),
        pk_b=pltpu.VMEM((2, rows // LANES, LANES), F32),
        pk_c=pltpu.VMEM((2, rows // LANES, LANES), F32),
        pk_d=pltpu.VMEM((2, rows // LANES, LANES), F32),
        tapf=pltpu.VMEM((cblocks, ntaps, LANES), F32),
        tapacc=pltpu.VMEM((cblocks, ntaps, 8, LANES), F32),
        rowacc=pltpu.VMEM((2, 8, chan), F32),
        gx=pltpu.VMEM((cblocks, HALO + rows, LANES), F32),
        gate_out=pltpu.VMEM((HALO, chan), BF16),
        gate_in=pltpu.VMEM((HALO, chan), BF16),
        halo_out=pltpu.VMEM((cblocks, HALO, LANES), BF16),
        halo_in=pltpu.VMEM((cblocks, HALO, LANES), BF16),
        acc_a=pltpu.VMEM((NX, NZ, 4, block, gcols), F32),
        acc_b=pltpu.VMEM((NY, NZ, 4, block, gcols), F32),
        acc_c=pltpu.VMEM((NZ, NY, 4, block, gcols), F32),
        sent_a=ring_buffer(NX, NZ),
        sent_b=ring_buffer(NY, NZ),
        sent_c=ring_buffer(NZ, NY),
        came_a=ring_buffer(NX, NZ),
        came_b=ring_buffer(NY, NZ),
        came_c=ring_buffer(NZ, NY),
        sent2_a=pieces(2, 3, NZ // 2),
        sent2_b=pieces(2, 3, NZ // 2),
        came2_a=pieces(2, 3, NZ // 2),
        came2_b=pieces(2, 3, NZ // 2),
        line=pltpu.VMEM((2, NZ, block, gcols), F32),
        sent3_a=pieces(NZ - 1),
        sent3_b=pieces(NZ - 1),
        came3_a=pieces(NZ - 1),
        came3_b=pieces(NZ - 1),
        sent_p=pieces(PLANE - 1),
        came_p=pieces(PLANE - 1),
        flat=pltpu.VMEM((PLANE * share, LANES), F32),
        packed=pltpu.VMEM((PLANE * share, LANES), BF16),
        parts=pltpu.VMEM((2, PLANE, share, LANES), BF16),
        pile=pltpu.VMEM((NZ, 2, share, LANES), BF16),
        final=pltpu.VMEM((2, share, LANES), BF16),
        whole=pltpu.VMEM((PLANE, share, LANES), BF16),
        in_sem=dma((8,)),
        tp_send=dma((2,)),
        tp_recv=dma((2,)),
        halo_send=dma,
        halo_recv=dma,
        ring_send=dma((GROUPS,)),
        ring_recv=dma((2 * (NX + NY + NZ) - 6,)),
        second_send=dma((2,)),
        second_recv=dma((2, 2)),
        third_send=dma((2,)),
        third_recv=dma((2,)),
        plane_send=dma,
        plane_recv=dma,
        gate_send=dma,
        gate_recv=dma,
        a_send=dma,
        a_recv=dma((2,)),
        b_send=dma,
        b_recv=dma,
        c_send=dma,
        c_recv=dma,
    )
    ins = ("cv_hbm", "cg_hbm", "co_hbm", "taps_hbm", "gain_hbm", "shift_hbm", "w_hbm", "og_hbm")
    outs = dict(
        gv=((rows, chan), BF16),
        gg=((rows, chan), BF16),
        taps_out=((ntaps, chan), F32),
        gain_out=((chan,), F32),
        shift_out=((chan,), F32),
        proj_out=((block, chan), F32),
    )
    results = pl.pallas_call(
        functools.partial(kernel, (*ins, *outs, *scratch)),
        out_shape=[pltpu.VMEM(*out) for out in outs.values()],
        in_specs=[pl.BlockSpec(memory_space=pltpu.HBM)] * 8,
        out_specs=[vmem] * len(outs),
        scratch_shapes=list(scratch.values()),
        compiler_params=pltpu.CompilerParams(
            collective_id=0, has_side_effects=True, vmem_limit_bytes=VMEM_LIMIT
        ),
    )(
        *[
            pltpu.with_memory_space_constraint(v, pltpu.HBM)
            for v in (
                conv_value, conv_gate, conv_out, conv_taps, norm_gain, norm_shift, proj_weight, out_grad,
            )
        ]
    )
    return pl.pallas_call(
        place,
        out_shape=[jax.ShapeDtypeStruct(*out) for out in outs.values()],
        in_specs=[vmem] * len(outs),
        out_specs=[hbm] * len(outs),
        scratch_shapes=[dma((len(outs),))],
        compiler_params=pltpu.CompilerParams(vmem_limit_bytes=1024 * 1024),
    )(*[pltpu.with_memory_space_constraint(v, pltpu.VMEM) for v in results])


def solution(mesh):
    in_specs = (
        P("sp", "tp"),
        P("sp", "tp"),
        P("sp", "tp"),
        P(None, "tp"),
        P("tp"),
        P("tp"),
        P(None, "tp"),
        P("sp", None),
    )
    out_specs = (P("sp", "tp"), P("sp", "tp"), P(None, "tp"), P("tp"), P("tp"), P("sp", "tp"))
    return jax.shard_map(local, mesh=mesh, in_specs=in_specs, out_specs=out_specs, check_vma=False)
```
